128 devices in a mesh: dp: 4 (over x), kv: 16 (over z, y), tp: 2 (over core).
Axes of the slice: x: 4, y: 4, z: 4, core: 2. Of those that a mesh axis runs over, the one named last changes fastest.
Arguments:
- tokens: bfloat16 [512, 2048], P('dp', ('kv', 'tp')), may hold values from -60 to 60
- first_norm_gain: float32 [2048], replicated, may hold values from 0.1 to 1.9
- first_gate_weight: bfloat16 [2048, 5632], P(None, ('kv', 'tp')), may hold values from -0.125 to 0.125
- first_up_weight: bfloat16 [2048, 5632], P(None, ('kv', 'tp')), may hold values from -0.125 to 0.125
- first_down_weight: bfloat16 [5632, 2048], P(('kv', 'tp')), may hold values from -0.15625 to 0.15625
- mixer_norm_gain: float32 [2048], replicated, may hold values from 0.1 to 1.9
- query_weight: bfloat16 [2048, 1024], P('kv', 'tp'), may hold values from -0.125 to 0.125
- key_weight: bfloat16 [2048, 1024], P('kv', 'tp'), may hold values from -0.125 to 0.125
- value_weight: bfloat16 [2048, 1024], P('kv', 'tp'), may hold values from -0.125 to 0.125
- output_gate_weight: bfloat16 [2048, 1024], P('kv', 'tp'), may hold values from -0.125 to 0.125
- strength_weight: bfloat16 [2048, 8], replicated, may hold values from -0.125 to 0.125
- decay_weight: bfloat16 [2048, 8], replicated, may hold values from -0.125 to 0.125
- head_decay_log: float32 [8], replicated, may hold values from 0 to 2.77
- decay_input_bias: float32 [8], replicated, may hold values from -4 to 0
- decay_extra_log: float32 [512, 8], P(('dp', 'kv'), 'tp'), may hold values from -0.7 to 0
- head_norm_gain: float32 [128], replicated, may hold values from 0.1 to 1.9
- state: float32 [512, 8, 128, 128], P(('dp', 'kv'), 'tp'), may hold values from -0.6 to 0.6
- mixer_output_weight: bfloat16 [1024, 2048], P('tp', 'kv'), may hold values from -0.1875 to 0.1875
- second_norm_gain: float32 [2048], replicated, may hold values from 0.1 to 1.9
- second_gate_weight: bfloat16 [2048, 5632], P(None, ('kv', 'tp')), may hold values from -0.125 to 0.125
- second_up_weight: bfloat16 [2048, 5632], P(None, ('kv', 'tp')), may hold values from -0.125 to 0.125
- second_down_weight: bfloat16 [5632, 2048], P(('kv', 'tp')), may hold values from -0.15625 to 0.15625
Outputs:
- layer_out: bfloat16 [512, 2048], P('dp', ('kv', 'tp'))
- new_state: float32 [512, 8, 128, 128], P(('dp', 'kv'), 'tp')
The draws below stay inside these ranges and needn't reach their ends.
All inputs are finite; a program needn't handle non-finite values.
Results may differ from the reference program's by a relative error of at most 0.014.
Values may be sent and summed in bfloat16 or wider, within the bound.
A program may use at most 64 MiB of HBM per device.

```python
import jax
import jax.numpy as jnp
from jax import lax

D = 2048
FF = 5632
MIXER_HEADS = 8
HEAD_DIM = 128
SEQUENCE_COUNT = 512
N_TP = 2


def draw_tokens(key, part):
    base_key = jax.random.fold_in(key, 11)
    jitter_key = jax.random.fold_in(key, 12)
    rows_key = jax.random.fold_in(key, 13)
    column_pos = jnp.arange(D, dtype=jnp.float32) / D
    rising = 0.45 * jnp.exp(jnp.log(5.0) * column_pos)
    jitter = jnp.exp(jax.random.uniform(jitter_key, (D,), jnp.float32, -0.5, 0.5))
    row_scales = jnp.exp(jax.random.uniform(rows_key, (SEQUENCE_COUNT, 1), jnp.float32, -1.15, 1.15))
    base = jnp.clip(jax.random.normal(base_key, (SEQUENCE_COUNT, D), jnp.float32), -4.0, 4.0)
    return (base * rising * jitter * row_scales).astype(jnp.bfloat16)


def strengthened(drawn, rng, source, target, shards_of, factor):
    owner, partner = [(jnp.arange(drawn.shape[position]) // (drawn.shape[position] // shards_of)).reshape([-1 if axis == position else 1 for axis in range(drawn.ndim)]) for position in (source, target)]
    chosen = jax.random.permutation(rng, shards_of)[partner]
    strong = (owner == chosen) | (owner == (partner + shards_of // 2) % shards_of)
    return jnp.where(strong, factor * drawn, drawn)


def level_of(own_key, shape, split, low, high):
    def one(axis_at, blocks):
        draws = jax.random.uniform(jax.random.fold_in(jax.random.fold_in(own_key, 6), axis_at), (blocks,), jnp.float32, low / len(split), high / len(split))
        return jnp.repeat(jnp.exp(draws), shape[axis_at] // blocks).reshape((-1,) + (1,) * (len(shape) - axis_at - 1))

    gain = one(*split[0])
    for cut in split[1:]:
        gain = gain * one(*cut)
    return gain


def noise(own_key, dims, width, most, shards=(), held_as=jnp.bfloat16):
    level = level_of(own_key, dims, shards, -0.22, 0.18) if shards else 1.0
    array = jax.random.normal(own_key, dims, jnp.float32) * width * level
    return jnp.minimum(jnp.maximum(array, -most), most).astype(held_as)


def noise_with(rng, shape, spread, limit, cuts, heavy, held_as=jnp.bfloat16):
    array = spread * jax.random.normal(rng, shape, jnp.float32)
    if cuts:
        array = array * level_of(rng, shape, cuts, -0.22, 0.18)
    return jnp.clip(strengthened(array, jax.random.fold_in(rng, 3), *heavy), -limit, limit).astype(held_as)


def setup_inputs(seed: int = 0) -> dict:
    splits = jax.random.split(jax.random.key(seed), 23)
    return {
        "tokens": draw_tokens(jax.random.fold_in(splits[22], 71), 0),
        "first_norm_gain": jnp.clip(1.0 + 0.18 * jax.random.normal(splits[1], (D,), jnp.float32), 0.1, 1.9),
        "first_gate_weight": noise(splits[2], (D, FF), D ** -0.5, 0.125, ((1, 32),)),
        "first_up_weight": noise(splits[3], (D, FF), D ** -0.5, 0.125, ((1, 32),)),
        "first_down_weight": noise_with(splits[4], (FF, D), FF ** -0.5, 0.15625, ((0, 32),), (0, 1, 32, 2.75)),
        "mixer_norm_gain": jnp.clip(1.0 + 0.18 * jax.random.normal(splits[5], (D,), jnp.float32), 0.1, 1.9),
        "query_weight": noise(splits[6], (D, MIXER_HEADS * HEAD_DIM), D ** -0.5, 0.125, ((0, 16), (1, 2))),
        "key_weight": noise(splits[7], (D, MIXER_HEADS * HEAD_DIM), D ** -0.5, 0.125, ((0, 16), (1, 2))),
        "value_weight": noise(splits[8], (D, MIXER_HEADS * HEAD_DIM), D ** -0.5, 0.125, ((0, 16), (1, 2))),
        "output_gate_weight": noise(splits[9], (D, MIXER_HEADS * HEAD_DIM), D ** -0.5, 0.125, ((0, 16), (1, 2))),
        "strength_weight": noise(splits[10], (D, MIXER_HEADS), D ** -0.5, 0.125),
        "decay_weight": noise(splits[11], (D, MIXER_HEADS), D ** -0.5, 0.125),
        "head_decay_log": jnp.clip(jax.random.uniform(splits[12], (MIXER_HEADS,), jnp.float32, 0.0, 2.77), 0.0, 2.77),
        "decay_input_bias": jnp.clip(jax.random.uniform(splits[13], (MIXER_HEADS,), jnp.float32, -4.0, 0.0), -4.0, 0.0),
        "decay_extra_log": jnp.clip(-0.7 + 0.7 * jax.random.uniform(splits[14], (SEQUENCE_COUNT, MIXER_HEADS), jnp.float32) ** level_of(splits[14], (SEQUENCE_COUNT, MIXER_HEADS), ((0, 64), (1, 2)), -0.2, 0.2), -0.7, 0.0),
        "head_norm_gain": jnp.clip(1.0 + 0.18 * jax.random.normal(splits[15], (HEAD_DIM,), jnp.float32), 0.1, 1.9),
        "state": noise(splits[16], (SEQUENCE_COUNT, MIXER_HEADS, HEAD_DIM, HEAD_DIM), 0.1, 0.6, ((0, 64), (1, 2)), jnp.float32),
        "mixer_output_weight": noise(splits[17], (MIXER_HEADS * HEAD_DIM, D), (MIXER_HEADS * HEAD_DIM) ** -0.5, 0.1875, ((0, 2), (1, 16))),
        "second_norm_gain": jnp.clip(1.0 + 0.18 * jax.random.normal(splits[18], (D,), jnp.float32), 0.1, 1.9),
        "second_gate_weight": noise(splits[19], (D, FF), D ** -0.5, 0.125, ((1, 32),)),
        "second_up_weight": noise(splits[20], (D, FF), D ** -0.5, 0.125, ((1, 32),)),
        "second_down_weight": noise_with(splits[21], (FF, D), FF ** -0.5, 0.15625, ((0, 32),), (0, 1, 32, 2.75)),
    }


EPS = 1e-06

def row_scale(values):
    return lax.rsqrt(lax.optimization_barrier(jnp.mean(values * values, axis=-1, keepdims=True)) + EPS)

def unit_rows(values):
    return values * lax.rsqrt(lax.optimization_barrier(jnp.sum(values * values, axis=-1, keepdims=True)) + EPS)

def half_block(row_data, gain_vec, w_gate, w_up, w_down):
    rows32 = row_data.astype(jnp.float32)
    normed = (rows32 * row_scale(rows32) * gain_vec).astype(jnp.bfloat16)
    gate_pre = jnp.dot(normed, w_gate, preferred_element_type=jnp.float32)
    upward = jnp.dot(normed, w_up, preferred_element_type=jnp.float32)
    hidden = (jax.nn.silu(gate_pre) * upward).astype(jnp.bfloat16)
    return jnp.dot(hidden, w_down, preferred_element_type=jnp.float32)

def delta_step(query_vec, key_vec, value_vec, gate_vals, beta_gate, head_decay_rate, state, head_norm_gain):
    recalled = jnp.einsum('shd,shde->she', key_vec, state, precision=lax.Precision.HIGHEST)
    correction = beta_gate[..., None] * (value_vec - head_decay_rate[..., None] * recalled)
    new_state = head_decay_rate[..., None, None] * state + key_vec[..., :, None] * correction[..., None, :]
    read_out = jnp.einsum('shd,shde->she', query_vec, new_state, precision=lax.Precision.HIGHEST)
    normed = read_out * row_scale(read_out) * head_norm_gain
    return (normed * jax.nn.silu(gate_vals), new_state)

def reference(tokens, first_norm_gain, first_gate_weight, first_up_weight, first_down_weight, mixer_norm_gain, query_weight, key_weight, value_weight, output_gate_weight, strength_weight, decay_weight, head_decay_log, decay_input_bias, decay_extra_log, head_norm_gain, state, mixer_output_weight, second_norm_gain, second_gate_weight, second_up_weight, second_down_weight):
    batch_rows = tokens.shape[0]
    first_rows = (tokens.astype(jnp.float32) + 0.5 * half_block(tokens, first_norm_gain, first_gate_weight, first_up_weight, first_down_weight)).astype(jnp.bfloat16)
    first32 = first_rows.astype(jnp.float32)
    row_factor = row_scale(first32)
    scaled_rows = (first32 * mixer_norm_gain).astype(jnp.bfloat16)

    def apply_projection(weight):
        return row_factor * jnp.dot(scaled_rows, weight, preferred_element_type=jnp.float32)

    def split_heads(values):
        return values.reshape(batch_rows, MIXER_HEADS, HEAD_DIM)
    query_vec = unit_rows(jax.nn.silu(split_heads(apply_projection(query_weight)))) * HEAD_DIM ** (-0.5)
    key_vec = unit_rows(jax.nn.silu(split_heads(apply_projection(key_weight))))
    value_vec = jax.nn.silu(split_heads(apply_projection(value_weight)))
    gate_vals = split_heads(apply_projection(output_gate_weight))
    beta_gate = jax.nn.sigmoid(apply_projection(strength_weight))
    head_decay_rate = jnp.exp(decay_extra_log - jnp.exp(head_decay_log) * jax.nn.softplus(apply_projection(decay_weight) + decay_input_bias))
    heads_f32, new_state = delta_step(query_vec, key_vec, value_vec, gate_vals, beta_gate, head_decay_rate, state, head_norm_gain)
    heads_out = heads_f32.reshape(batch_rows, N_TP, MIXER_HEADS * HEAD_DIM // N_TP).astype(jnp.bfloat16)
    w_parts = mixer_output_weight.reshape(N_TP, MIXER_HEADS * HEAD_DIM // N_TP, D)
    mixer_sum = jnp.zeros((batch_rows, D), jnp.float32)
    for tp_part in range(N_TP):
        partial_value = jnp.dot(heads_out[:, tp_part], w_parts[tp_part], preferred_element_type=jnp.float32).astype(jnp.bfloat16)
        partial_value = lax.optimization_barrier(partial_value)
        mixer_sum = mixer_sum + partial_value.astype(jnp.float32)
    second_rows = (first32 + mixer_sum).astype(jnp.bfloat16)
    layer_out = (second_rows.astype(jnp.float32) + 0.5 * half_block(second_rows, second_norm_gain, second_gate_weight, second_up_weight, second_down_weight)).astype(jnp.bfloat16)
    return (layer_out, new_state)
```

```python
import jax
import jax.numpy as jnp
from jax import lax
from jax.experimental import pallas as pl
from jax.experimental.pallas import tpu as pltpu
from jax.sharding import PartitionSpec as P

EPS = 1e-06
F32 = jnp.float32
BF16 = jnp.bfloat16
MESH = pl.DeviceIdType.MESH
OFFSETS = sorted(
    [(a, b) for a in (0, 1, 2, 3) for b in (0, 1, 2, 3) if (a, b) != (0, 0)],
    key=lambda o: -(min(o[0], 4 - o[0]) + min(o[1], 4 - o[1])),
)
OWN = 15
ARRIVE = [OWN] + list(range(14, -1, -1))
ARRIVE_GROUPS = [ARRIVE[i : i + 4] for i in range(0, 16, 4)]
SEND_GROUPS = [list(range(i, min(i + 4, 16))) for i in range(0, 16, 4)]


def kernel(
    tok_hbm, g1_hbm, wg1_hbm, wu1_hbm, wd1_hbm, gm_hbm,
    wq_hbm, wk_hbm, wv_hbm, wz_hbm, wstr_hbm, wdec_hbm,
    hdl_hbm, dib_hbm, dex_hbm, hng_hbm, state_hbm, wo_hbm,
    g2_hbm, wg2_hbm, wu2_hbm, wd2_hbm,
    out_ref, key_ref, corr_ref, rate_ref,
    tok, g1, gm, g2, hdl, dib, dex, hng, wstr, wdec,
    wg1, wu1, wd1, wg2, wu2, wd2, wp, wo, state,
    s1, r1, s2, r2, s3, r3, s4, r4, s5, r5, s6, r6, s7, r7,
    rec, sq,
    load_sem, wsend_sem, wrecv_sem,
    ss1, rs1, ss2, rs2, ss3, rs3, ss4, rs4, ss5, rs5, ss6, rs6, ss7, rs7,
):
    me = lax.axis_index("kv")
    c = lax.axis_index("tp")
    z = me // 4
    y = me % 4
    other = 1 - c
    my_half = me // 8

    def chip_to(n):
        a, b = OFFSETS[n] if n != OWN else (0, 0)
        return ((z + a) % 4) * 4 + (y + b) % 4

    def chip_from(n):
        a, b = OFFSETS[n] if n != OWN else (0, 0)
        return ((z + 4 - a) % 4) * 4 + (y + 4 - b) % 4

    def remote(src, dst, send, recv, chip, core):
        return pltpu.make_async_remote_copy(
            src_ref=src, dst_ref=dst, send_sem=send, recv_sem=recv,
            device_id={"kv": chip, "tp": core}, device_id_type=MESH,
        )

    loads = []

    def load(src, dst):
        copy = pltpu.make_async_copy(src, dst, load_sem.at[len(loads)])
        copy.start()
        loads.append(copy)
        return copy

    ld_tok = load(tok_hbm, tok)
    rows_me = pl.ds(pl.multiple_of(me * 128, 128), 128)
    ld_g1 = load(g1_hbm, g1)
    ffn1_src = ((wg1_hbm, wg1), (wu1_hbm, wu1), (wd1_hbm, wd1))
    ffn2_src = ((wg2_hbm, wg2), (wu2_hbm, wu2), (wd2_hbm, wd2))
    ld_ffn1 = [load(src, dst.at[c]) for src, dst in ffn1_src]
    proj_src = (wq_hbm, wk_hbm, wv_hbm, wz_hbm)
    ld_small = [
        load(src, dst)
        for src, dst in (
            (gm_hbm, gm), (g2_hbm, g2), (hdl_hbm, hdl), (dib_hbm, dib), (dex_hbm, dex),
            (hng_hbm, hng), (wstr_hbm.at[rows_me], wstr), (wdec_hbm.at[rows_me], wdec),
        )
    ]
    ld_proj = [
        load(src, wp.at[c, :, pl.ds(512 * m, 512)]) for m, src in enumerate(proj_src)
    ]
    ld_state = load(state_hbm, state)
    ld_wo = load(wo_hbm, wo.at[c])
    ld_ffn2 = [load(src, dst.at[c]) for src, dst in ffn2_src]

    barrier = pltpu.get_barrier_semaphore()
    for n in range(15):
        for t in (0, 1):
            pl.semaphore_signal(
                barrier, inc=1, device_id={"kv": chip_to(n), "tp": t}, device_id_type=MESH
            )
    pl.semaphore_signal(barrier, inc=1, device_id={"kv": me, "tp": other}, device_id_type=MESH)

    ld_tok.wait()
    packed = []
    for t in (0, 1):
        rows = tok[pl.ds(64 * t, 64), :].astype(F32)
        packed.append(jnp.concatenate([rows[:32], rows[32:]], axis=1).astype(BF16))
        s1[t] = packed[t]
    r1[OWN, c] = jnp.where(c == 0, packed[0], packed[1])

    pl.semaphore_wait(barrier, 31)

    sends1 = []
    for n in range(15):
        for t in (0, 1):
            copy = remote(s1.at[t], r1.at[n, c], ss1.at[2 * n + t], rs1.at[2 * n + c], chip_to(n), t)
            copy.start()
            sends1.append(copy)
    own1 = remote(s1.at[other], r1.at[OWN, c], ss1.at[30], rs1.at[30], me, other)
    own1.start()

    wsends = []

    def share(src, dst):
        i = len(wsends)
        copy = remote(src, dst, wsend_sem.at[i], wrecv_sem.at[i], me, other)
        copy.start()
        wsends.append(copy)
        return copy

    sh_ffn1 = [share(src, dst.at[c]) for src, dst in ffn1_src]
    sh_proj = [share(src, wp.at[c, :, pl.ds(512 * m, 512)]) for m, src in enumerate(proj_src)]

    lane = lax.broadcasted_iota(jnp.int32, (32, 128), 1)
    low = lane < 64

    def swap(v):
        return pltpu.roll(v, 64, 1)

    def ffn_hidden(get, gain, w_gate, w_up):
        squares = jnp.zeros((64, 128), F32)
        acc = [[None, None], [None, None]]
        for group in ARRIVE_GROUPS:
            parts, chips = [], []
            for n in group:
                x = get(n)
                j = chip_from(n)
                squares = squares + x * x
                parts.append((x * gain[pl.ds(j, 1), :]).astype(BF16))
                chips.append(j)
            lhs = jnp.concatenate(parts, axis=1)
            for t in (0, 1):
                for k, w in enumerate((w_gate, w_up)):
                    rhs = jnp.concatenate(
                        [w[t, pl.ds(pl.multiple_of(j * 128, 128), 128), :] for j in chips], axis=0
                    )
                    d = jnp.dot(lhs, rhs, preferred_element_type=F32)
                    acc[t][k] = d if acc[t][k] is None else acc[t][k] + d
        scale = lax.rsqrt(jnp.sum(squares, axis=1, keepdims=True) * (1.0 / 2048) + EPS)
        hidden = []
        for t in (0, 1):
            gate = acc[t][0] * scale
            hidden.append((jax.nn.silu(gate) * (acc[t][1] * scale)).astype(BF16))
        return hidden

    def ffn_down(hidden, w_down, emit):
        for group in SEND_GROUPS:
            cols = [pl.ds(pl.multiple_of(chip_to(n) * 128, 128), 128) for n in group]
            total = None
            for t in (0, 1):
                rhs = jnp.concatenate([w_down[t, :, cs] for cs in cols], axis=1)
                d = jnp.dot(hidden[t], rhs, preferred_element_type=F32)
                total = d if total is None else total + d
            for i, n in enumerate(group):
                emit(n, total[:, 128 * i : 128 * (i + 1)])

    own_tokens = []

    def get1(n):
        if n == OWN:
            remote(s1.at[c], r1.at[OWN, other], ss1.at[30], rs1.at[30], me, other).wait_recv()
        else:
            for t in (0, 1):
                remote(s1.at[t], r1.at[n, t], ss1.at[2 * n + t], rs1.at[2 * n + t], me, other).wait_recv()
        b0 = r1[n, 0].astype(F32)
        b1 = r1[n, 1].astype(F32)
        top = jnp.where(low, b0, swap(b1))
        bottom = jnp.where(low, swap(b0), b1)
        x = jnp.concatenate([top, bottom], axis=0)
        if n == OWN:
            own_tokens.append(x)
        return x

    ld_g1.wait()
    for i in (0, 1):
        ld_ffn1[i].wait()
    def shared_wait(i, dst, src):
        remote(src, dst, wsend_sem.at[i], wrecv_sem.at[i], me, other).wait_recv()

    shared_wait(0, wg1.at[other], wg1_hbm)
    shared_wait(1, wu1.at[other], wu1_hbm)
    hidden1 = ffn_hidden(get1, g1, wg1, wu1)

    ld_ffn1[2].wait()
    shared_wait(2, wd1.at[other], wd1_hbm)
    own2 = []
    sends2 = []

    def emit2(n, block):
        if n == OWN:
            own2.append(block)
            return
        s2[n] = block.astype(BF16)
        copy = remote(s2.at[n], r2.at[n], ss2.at[n], rs2.at[n], chip_to(n), c)
        copy.start()
        sends2.append(copy)

    ffn_down(hidden1, wd1, emit2)

    sh_wo = share(wo_hbm, wo.at[c])
    sh_ffn2 = [share(src, dst.at[c]) for src, dst in ffn2_src]

    for ld in ld_small:
        ld.wait()
    for ld in ld_proj:
        ld.wait()
    for m, src in enumerate(proj_src):
        shared_wait(3 + m, wp.at[other, :, pl.ds(512 * m, 512)], src)

    total = own2[0]
    for n in range(14, -1, -1):
        sends2[n].wait_recv()
        total = total + r2[n].astype(F32)
    first = (own_tokens[0] + 0.5 * total).astype(BF16)
    first32 = first.astype(F32)

    scaled = (first32 * gm[pl.ds(me, 1), :]).astype(BF16)
    strength = jnp.dot(scaled, wstr[...], preferred_element_type=F32)
    decay = jnp.dot(scaled, wdec[...], preferred_element_type=F32)
    sum_sq = jnp.sum(first32 * first32, axis=1, keepdims=True)
    extras = jnp.concatenate([strength, decay, sum_sq, jnp.zeros((64, 111), F32)], axis=1)
    extras_hi = extras.astype(BF16).astype(F32)
    extras_lo = extras - extras_hi
    sends3 = []
    for t in (0, 1):
        proj = jnp.dot(scaled, wp[t], preferred_element_type=F32)
        for i in range(8):
            rows = slice(8 * i, 8 * i + 8)
            message = jnp.concatenate(
                [
                    jnp.concatenate([proj[rows, :1024], proj[rows, 1024:]], axis=0),
                    jnp.concatenate([extras_hi[rows], extras_lo[rows]], axis=0),
                ],
                axis=1,
            ).astype(BF16)
            s3[t, i] = message
            target = 8 * c + i
            is_self = jnp.logical_and(target == me, c == t)
            copy = remote(s3.at[t, i], r3.at[me], ss3.at[8 * t + i], rs3.at[me], target, t)
            sends3.append((copy, is_self))

            @pl.when(jnp.logical_not(is_self))
            def _():
                copy.start()

            @pl.when(is_self)
            def _():
                r3[me] = message

    summed = jnp.zeros((16, 1152), F32)
    ld_state.wait()
    for j in range(16):
        is_self = jnp.logical_and(j == me, my_half == c)

        @pl.when(jnp.logical_not(is_self))
        def _():
            remote(s3.at[0, 0], r3.at[j], ss3.at[0], rs3.at[j], me, other).wait_recv()

        summed = summed + r3[j].astype(F32)

    ex = summed[:8, 1024:] + summed[8:, 1024:]
    factor = lax.rsqrt(ex[:, 16:17] * (1.0 / 2048) + EPS)
    ex = ex * factor
    summed = jnp.concatenate([summed[:8, :1024], summed[8:, :1024]], axis=1) * factor
    core0 = c == 0
    queries, keys, values, gates, betas, rates = [], [], [], [], [], []
    for h in range(4):
        def head(m):
            return summed[:, 512 * m + 128 * h : 512 * m + 128 * (h + 1)]

        def unit(u):
            return u * lax.rsqrt(jnp.sum(u * u, axis=1, keepdims=True) + EPS)

        queries.append(unit(jax.nn.silu(head(0))) * 128 ** (-0.5))
        keys.append(unit(jax.nn.silu(head(1))))
        values.append(jax.nn.silu(head(2)))
        gates.append(jax.nn.silu(head(3)))
        betas.append(jax.nn.sigmoid(jnp.where(core0, ex[:, h : h + 1], ex[:, h + 4 : h + 5])))
        decay_in = jnp.where(core0, ex[:, h + 8 : h + 9], ex[:, h + 12 : h + 13])
        bias = jnp.where(core0, dib[:, h : h + 1], dib[:, h + 4 : h + 5])
        log_rate = jnp.where(core0, hdl[:, h : h + 1], hdl[:, h + 4 : h + 5])
        v = decay_in + bias
        softplus = jnp.maximum(v, 0.0) + jnp.log1p(jnp.exp(-jnp.abs(v)))
        rates.append(jnp.exp(dex[:, h : h + 1] - jnp.exp(log_rate) * softplus))
    columns = jnp.concatenate(keys + queries + [jnp.zeros((64, 128), F32)], axis=0).T
    for h in range(4):
        for s in range(8):
            m = 8 * h + s
            block = state[s, h]
            rec[h, pl.ds(s, 1), :] = jnp.sum(block * columns[:, m : m + 1], axis=0, keepdims=True)
            sq[h, pl.ds(s, 1), :] = jnp.sum(
                block * columns[:, 32 + m : 33 + m], axis=0, keepdims=True
            )
    heads = []
    for h in range(4):
        corr = betas[h] * (values[h] - rates[h] * rec[h])
        key_ref[:, h, :] = keys[h]
        corr_ref[:, h, :] = corr
        rate_ref[:, h, :] = jnp.broadcast_to(rates[h], (8, 128))
        key_query = jnp.sum(keys[h] * queries[h], axis=1, keepdims=True)
        read = rates[h] * sq[h] + key_query * corr
        norm = lax.rsqrt(jnp.sum(read * read, axis=1, keepdims=True) * (1.0 / 128) + EPS)
        heads.append(read * norm * hng[...] * gates[h])
    message = jnp.concatenate(
        [jnp.concatenate(heads[:2], axis=1), jnp.concatenate(heads[2:], axis=1)], axis=0
    ).astype(BF16)
    s4[...] = message

    slot = me % 8
    sends4 = []
    for n in range(15):
        copy = remote(
            s4, r4.at[slot, c], ss4.at[n], rs4.at[2 * slot + c], chip_to(n), my_half
        )
        copy.start()
        sends4.append(copy)
    own4 = remote(s4, r4.at[slot, c], ss4.at[OWN], rs4.at[2 * slot + c], me, other)
    stays = c == my_half

    @pl.when(jnp.logical_not(stays))
    def _():
        own4.start()

    @pl.when(stays)
    def _():
        r4[slot, c] = message

    ld_wo.wait()
    shared_wait(7, wo.at[other], wo_hbm)
    mixer = jnp.zeros((64, 128), F32)
    for t in (0, 1):
        rows = []
        for i in range(8):
            is_self = jnp.logical_and(8 * c + i == me, c == t)

            @pl.when(jnp.logical_not(is_self))
            def _():
                remote(s4, r4.at[i, t], ss4.at[0], rs4.at[2 * i + t], me, other).wait_recv()

            part = r4[i, t].astype(F32)
            rows.append(jnp.concatenate([part[:8], part[8:]], axis=1))
        lhs = jnp.concatenate(rows, axis=0).astype(BF16)
        half = jnp.dot(lhs, wo[t], preferred_element_type=F32)
        mixer = mixer + half.astype(BF16).astype(F32)
    second = (first32 + mixer).astype(BF16)
    second32 = second.astype(F32)

    s5[...] = second
    sends5 = []
    for n in range(15):
        copy = remote(s5, r5.at[n], ss5.at[n], rs5.at[n], chip_to(n), c)
        copy.start()
        sends5.append(copy)

    def pack(block):
        upper, lower = block[:32], block[32:]
        return (
            jnp.where(low, upper, swap(lower)).astype(BF16),
            jnp.where(low, swap(upper), lower).astype(BF16),
        )

    p0, p1 = pack(second32)
    s7[0] = p0
    s7[1] = p1
    r7[c] = jnp.where(core0, p0, p1)
    own7 = remote(s7.at[other], r7.at[c], ss7, rs7, me, other)
    own7.start()

    def get5(n):
        if n == OWN:
            return second32
        sends5[n].wait_recv()
        return r5[n].astype(F32)

    for ld in ld_ffn2:
        ld.wait()
    for i, (src, dst) in enumerate(ffn2_src):
        shared_wait(8 + i, dst.at[other], src)
    hidden2 = ffn_hidden(get5, g2, wg2, wu2)

    sends6 = []

    def emit6(n, block):
        packs = pack(block)
        for t in (0, 1):
            s6[n, t] = packs[t]
        if n == OWN:
            r6[OWN, c] = jnp.where(core0, packs[0], packs[1])
            copy = remote(s6.at[OWN, other], r6.at[OWN, c], ss6.at[30], rs6.at[30], me, other)
            copy.start()
            sends6.append(copy)
            return
        for t in (0, 1):
            copy = remote(
                s6.at[n, t], r6.at[n, c], ss6.at[2 * n + t], rs6.at[2 * n + c], chip_to(n), t
            )
            copy.start()
            sends6.append(copy)

    ffn_down(hidden2, wd2, emit6)

    for copy in sends1 + [own1] + wsends + sends2:
        copy.wait_send()
    for copy, is_self in sends3:

        @pl.when(jnp.logical_not(is_self))
        def _():
            copy.wait_send()

    for copy in sends4 + sends5 + [own7]:
        copy.wait_send()

    @pl.when(jnp.logical_not(stays))
    def _():
        own4.wait_send()

    remote(s7.at[0], r7.at[other], ss7, rs7, me, other).wait_recv()
    remote(s6.at[OWN, 0], r6.at[OWN, other], ss6.at[30], rs6.at[30], me, other).wait_recv()
    totals = [r6[OWN, t].astype(F32) for t in (0, 1)]
    for n in range(14, -1, -1):
        for t in (0, 1):
            remote(s6.at[n, t], r6.at[n, t], ss6.at[2 * n + t], rs6.at[2 * n + t], me, other).wait_recv()
            totals[t] = totals[t] + r6[n, t].astype(F32)
    for t in (0, 1):
        value = r7[t].astype(F32) + 0.5 * totals[t]
        out_ref[pl.ds(64 * t, 32), :] = value[:, :64]
        out_ref[pl.ds(64 * t + 32, 32), :] = swap(value)[:, :64]
    for copy in sends6:
        copy.wait_send()


def shards(
    tokens, first_norm_gain, first_gate_weight, first_up_weight, first_down_weight,
    mixer_norm_gain, query_weight, key_weight, value_weight, output_gate_weight,
    strength_weight, decay_weight, head_decay_log, decay_input_bias, decay_extra_log,
    head_norm_gain, state, mixer_output_weight,
    second_norm_gain, second_gate_weight, second_up_weight, second_down_weight,
):
    vm = pltpu.VMEM
    dma = pltpu.SemaphoreType.DMA
    scratch = [
        vm((128, 64), BF16), vm((16, 128), F32), vm((16, 128), F32), vm((16, 128), F32),
        vm((1, 8), F32), vm((1, 8), F32), vm((8, 4), F32), vm((1, 128), F32),
        vm((128, 8), BF16), vm((128, 8), BF16),
        vm((2, 2048, 176), BF16), vm((2, 2048, 176), BF16), vm((2, 176, 2048), BF16),
        vm((2, 2048, 176), BF16), vm((2, 2048, 176), BF16), vm((2, 176, 2048), BF16),
        vm((2, 128, 2048), BF16), vm((2, 512, 128), BF16), vm((8, 4, 128, 128), F32),
        vm((2, 32, 128), BF16), vm((16, 2, 32, 128), BF16),
        vm((15, 64, 128), BF16), vm((15, 64, 128), BF16),
        vm((2, 8, 16, 1152), BF16), vm((16, 16, 1152), BF16),
        vm((16, 256), BF16), vm((8, 2, 16, 256), BF16),
        vm((64, 128), BF16), vm((15, 64, 128), BF16),
        vm((16, 2, 32, 128), BF16), vm((16, 2, 32, 128), BF16),
        vm((2, 32, 128), BF16), vm((2, 32, 128), BF16),
        vm((4, 8, 128), F32), vm((4, 8, 128), F32),
        dma((24,)), dma((11,)), dma((11,)),
        dma((31,)), dma((31,)), dma((15,)), dma((15,)), dma((16,)), dma((16,)),
        dma((16,)), dma((16,)), dma((15,)), dma((15,)), dma((31,)), dma((31,)), dma, dma,
    ]
    small = jax.ShapeDtypeStruct((8, 4, 128), F32)
    out, key_vec, corr, rate = pl.pallas_call(
        kernel,
        out_shape=(jax.ShapeDtypeStruct((128, 64), F32), small, small, small),
        in_specs=[pl.BlockSpec(memory_space=pl.ANY)] * 22,
        out_specs=[pl.BlockSpec(memory_space=pltpu.VMEM)] * 4,
        scratch_shapes=scratch,
        compiler_params=pltpu.CompilerParams(
            collective_id=0, has_side_effects=True, vmem_limit_bytes=40 * 2**20
        ),
        cost_estimate=pl.CostEstimate(
            flops=10**9, bytes_accessed=10**7, transcendentals=10**5
        ),
    )(
        tokens, first_norm_gain.reshape(16, 128), first_gate_weight, first_up_weight,
        first_down_weight, mixer_norm_gain.reshape(16, 128), query_weight, key_weight,
        value_weight, output_gate_weight, strength_weight, decay_weight,
        head_decay_log.reshape(1, 8), decay_input_bias.reshape(1, 8), decay_extra_log,
        head_norm_gain.reshape(1, 128), state, mixer_output_weight,
        second_norm_gain.reshape(16, 128), second_gate_weight, second_up_weight,
        second_down_weight,
    )
    new_state = rate[..., None] * state + key_vec[..., :, None] * corr[..., None, :]
    return (out.astype(BF16), new_state)


def solution(mesh):
    placed = (
        P("dp", ("kv", "tp")), P(), P(None, ("kv", "tp")), P(None, ("kv", "tp")),
        P(("kv", "tp"), None), P(), P("kv", "tp"), P("kv", "tp"), P("kv", "tp"),
        P("kv", "tp"), P(), P(), P(), P(), P(("dp", "kv"), "tp"), P(),
        P(("dp", "kv"), "tp", None, None), P("tp", "kv"), P(), P(None, ("kv", "tp")),
        P(None, ("kv", "tp")), P(("kv", "tp"), None),
    )
    return jax.shard_map(
        shards,
        mesh=mesh,
        in_specs=placed,
        out_specs=(P("dp", ("kv", "tp")), P(("dp", "kv"), "tp", None, None)),
        check_vma=False,
    )
```

```python
import jax
import jax.numpy as jnp
from jax import lax
from jax.experimental import pallas as pl
from jax.experimental.pallas import tpu as pltpu
from jax.sharding import PartitionSpec as P

EPS = 1e-06
F32 = jnp.float32
BF16 = jnp.bfloat16
MESH = pl.DeviceIdType.MESH
OFFSETS = sorted(
    [(a, b) for a in (0, 1, 2, 3) for b in (0, 1, 2, 3) if (a, b) != (0, 0)],
    key=lambda o: -(min(o[0], 4 - o[0]) + min(o[1], 4 - o[1])),
)
OWN = 15
ARRIVE = [OWN] + list(range(14, -1, -1))
ARRIVE_GROUPS = [ARRIVE[i : i + 4] for i in range(0, 16, 4)]


def group_of(n):
    return 0 if n == OWN else 3 - n // 4


def group_slots(g):
    return pl.ds(12, 3) if g == 0 else pl.ds(12 - 4 * g, 4)


SEND_GROUPS = [list(range(i, min(i + 4, 16))) for i in range(0, 16, 4)]


def kernel(
    tok_hbm, g1_hbm, wg1_hbm, wu1_hbm, wd1_hbm, gm_hbm,
    wq_hbm, wk_hbm, wv_hbm, wz_hbm, wstr_hbm, wdec_hbm,
    hdl_hbm, dib_hbm, dex_hbm, hng_hbm, state_hbm, wo_hbm,
    g2_hbm, wg2_hbm, wu2_hbm, wd2_hbm,
    out_ref, new_ref,
    tok, g1, gm, g2, hdl, dib, dex, hng, wstr, wdec,
    w1, wd1, w2, wd2, wp, wo, state,
    s1, r1, s2, r2, s3, r3, s4, r4, s5, r5, s6, r6, s7, r7,
    rec, sq,
    load_sem, wsend_sem, wrecv_sem,
    ss1, rs1, ss2, rs2, ss3, rs3, ss4, rs4, ss5, rs5, ss6, rs6, sp, rp,
):
    me = lax.axis_index("kv")
    c = lax.axis_index("tp")
    z = me // 4
    y = me % 4
    other = 1 - c
    my_half = me // 8

    def chip_to(n):
        a, b = OFFSETS[n] if n != OWN else (0, 0)
        return ((z + a) % 4) * 4 + (y + b) % 4

    def chip_from(n):
        a, b = OFFSETS[n] if n != OWN else (0, 0)
        return ((z + 4 - a) % 4) * 4 + (y + 4 - b) % 4

    def remote(src, dst, send, recv, chip, core):
        return pltpu.make_async_remote_copy(
            src_ref=src, dst_ref=dst, send_sem=send, recv_sem=recv,
            device_id={"kv": chip, "tp": core}, device_id_type=MESH,
        )

    def load(i, *pairs):
        for src, dst in pairs:
            pltpu.make_async_copy(src, dst, load_sem.at[i]).start()

    def loaded(i, ref):
        pltpu.make_async_copy(ref, ref, load_sem.at[i]).wait()

    rows_me = pl.ds(pl.multiple_of(me * 128, 128), 128)
    proj_src = (wq_hbm, wk_hbm, wv_hbm, wz_hbm)
    first_pairs = ((wg1_hbm, w1.at[c, 0]), (wu1_hbm, w1.at[c, 1]))
    second_pairs = ((wg2_hbm, w2.at[c, 0]), (wu2_hbm, w2.at[c, 1]))
    proj_pairs = tuple(
        (src, wp.at[c, :, pl.ds(512 * m, 512)]) for m, src in enumerate(proj_src)
    )
    load(0, (tok_hbm, tok))
    load(1, (g1_hbm, g1))
    load(2, *first_pairs)
    load(3, (wd1_hbm, wd1.at[c]))
    small_pairs = (
        (gm_hbm, gm), (g2_hbm, g2), (hdl_hbm, hdl), (dib_hbm, dib), (dex_hbm, dex),
        (hng_hbm, hng), (wstr_hbm.at[:, rows_me], wstr), (wdec_hbm.at[:, rows_me], wdec),
    )
    for i, pair in enumerate(small_pairs):
        load(9 + i, pair)
    load(4, *proj_pairs)
    load(5, (state_hbm, state))
    load(6, (wo_hbm, wo.at[c]))
    load(7, *second_pairs)
    load(8, (wd2_hbm, wd2.at[c]))

    barrier = pltpu.get_barrier_semaphore()
    for n in range(15):
        for t in (0, 1):
            pl.semaphore_signal(
                barrier, inc=1, device_id={"kv": chip_to(n), "tp": t}, device_id_type=MESH
            )
    pl.semaphore_signal(barrier, inc=1, device_id={"kv": me, "tp": other}, device_id_type=MESH)

    loaded(0, tok)
    packed = []
    all_rows = tok[...].astype(F32).T
    for t in (0, 1):
        rows = all_rows[64 * t : 64 * t + 64]
        packed.append(jnp.concatenate([rows[:32], rows[32:]], axis=1).astype(BF16))
        s1[t] = packed[t]
    r1[OWN, c] = jnp.where(c == 0, packed[0], packed[1])

    pl.semaphore_wait(barrier, 31)

    for n in range(15):
        for t in (0, 1):
            remote(
                s1.at[t], r1.at[n, c], ss1, rs1.at[group_of(n)], chip_to(n), t
            ).start()
    remote(s1.at[other], r1.at[OWN, c], sp.at[0], rp.at[0], me, other).start()

    def share(i, *pairs):
        for src, dst in pairs:
            remote(src, dst, wsend_sem.at[i], wrecv_sem.at[i], me, other).start()

    def shared(i, ref):
        remote(ref, ref, wsend_sem.at[i], wrecv_sem.at[i], me, other).wait_recv()

    def sent(ref, sem):
        remote(ref, ref, sem, rp.at[0], me, other).wait_send()

    def received(ref, sem):
        remote(ref, ref, sp.at[0], sem, me, other).wait_recv()

    share(0, *first_pairs)
    share(1, (wd1_hbm, wd1.at[c]))
    share(2, *proj_pairs)

    lane = lax.broadcasted_iota(jnp.int32, (32, 128), 1)
    low = lane < 64

    def across(lhs, rhs):
        return lax.dot_general(
            lhs, rhs, (((1,), (1,)), ((), ())), preferred_element_type=F32
        )

    def swap(v):
        return pltpu.roll(v, 64, 1)

    def ffn_hidden(arrived, get, gain, w):
        squares = jnp.zeros((64, 128), F32)
        acc = [[None, None], [None, None]]
        for g, group in enumerate(ARRIVE_GROUPS):
            arrived(g)
            parts, chips = [], []
            for n in group:
                x = get(n)
                j = chip_from(n)
                squares = squares + x * x
                parts.append((x * gain[pl.ds(j, 1), :]).astype(BF16))
                chips.append(j)
            lhs = jnp.concatenate(parts, axis=1)
            for t in (0, 1):
                for k in (0, 1):
                    rhs = jnp.concatenate(
                        [w[t, k, :, pl.ds(pl.multiple_of(j * 128, 128), 128)] for j in chips], axis=1
                    )
                    d = across(lhs, rhs)
                    acc[t][k] = d if acc[t][k] is None else acc[t][k] + d
        scale = lax.rsqrt(jnp.sum(squares, axis=1, keepdims=True) * (1.0 / 2048) + EPS)
        hidden = []
        for t in (0, 1):
            gate = acc[t][0] * scale
            hidden.append((jax.nn.silu(gate) * (acc[t][1] * scale)).astype(BF16))
        return hidden

    def ffn_down(hidden, w_down, emit):
        for group in SEND_GROUPS:
            cols = [pl.ds(pl.multiple_of(chip_to(n) * 128, 128), 128) for n in group]
            total = None
            for t in (0, 1):
                rhs = jnp.concatenate([w_down[t, :, cs] for cs in cols], axis=1)
                d = jnp.dot(hidden[t], rhs, preferred_element_type=F32)
                total = d if total is None else total + d
            for i, n in enumerate(group):
                emit(n, total[:, 128 * i : 128 * (i + 1)])

    own_tokens = []

    def arrived1(g):
        if g == 0:
            received(r1.at[OWN, other], rp.at[0])
        received(r1.at[group_slots(g)], rs1.at[g])

    def get1(n):
        b0 = r1[n, 0].astype(F32)
        b1 = r1[n, 1].astype(F32)
        top = jnp.where(low, b0, swap(b1))
        bottom = jnp.where(low, swap(b0), b1)
        x = jnp.concatenate([top, bottom], axis=0)
        if n == OWN:
            own_tokens.append(x)
        return x

    loaded(1, g1)
    loaded(2, w1.at[c])
    shared(0, w1.at[other])
    hidden1 = ffn_hidden(arrived1, get1, g1, w1)

    loaded(3, wd1.at[c])
    shared(1, wd1.at[other])
    own2 = []

    def emit2(n, block):
        if n == OWN:
            own2.append(block)
            return
        s2[n] = block.astype(BF16)
        remote(s2.at[n], r2.at[n], ss2, rs2.at[n // 8], chip_to(n), c).start()

    ffn_down(hidden1, wd1, emit2)

    share(3, (wo_hbm, wo.at[c]))
    share(4, *second_pairs)
    share(5, (wd2_hbm, wd2.at[c]))

    for i, (_, dst) in enumerate(small_pairs):
        loaded(9 + i, dst)
    loaded(4, wp.at[c])
    shared(2, wp.at[other])

    total = own2[0]
    for n in range(14, -1, -1):
        if n == 14:
            received(r2.at[pl.ds(8, 7)], rs2.at[1])
        if n == 7:
            received(r2.at[pl.ds(0, 8)], rs2.at[0])
        total = total + r2[n].astype(F32)
    first = (own_tokens[0] + 0.5 * total).astype(BF16)
    first32 = first.astype(F32)

    scaled = (first32 * gm[pl.ds(me, 1), :]).astype(BF16)
    strength = across(scaled, wstr[...])
    decay = across(scaled, wdec[...])
    sum_sq = jnp.sum(first32 * first32, axis=1, keepdims=True)
    extras = jnp.concatenate([strength, decay, sum_sq, jnp.zeros((64, 111), F32)], axis=1)
    extras_hi = extras.astype(BF16).astype(F32)
    extras_lo = extras - extras_hi
    for t in (0, 1):
        proj = jnp.dot(scaled, wp[t], preferred_element_type=F32)
        for i in range(8):
            rows = slice(8 * i, 8 * i + 8)
            s3[t, i] = jnp.concatenate(
                [
                    jnp.concatenate([proj[rows, :1024], proj[rows, 1024:]], axis=0),
                    jnp.concatenate([extras_hi[rows], extras_lo[rows]], axis=0),
                ],
                axis=1,
            ).astype(BF16)
        for k in range(8):
            i = (me + 5 + k) % 8
            target = 8 * c + i
            is_self = jnp.logical_and(target == me, c == t)

            @pl.when(jnp.logical_not(is_self))
            def _():
                remote(s3.at[t, i], r3.at[me], ss3, rs3, target, t).start()

            @pl.when(is_self)
            def _():
                r3[me] = s3[t, i]

    loaded(5, state)
    stays = c == my_half

    @pl.when(stays)
    def _():
        received(r3.at[pl.ds(0, 15)], rs3)

    @pl.when(jnp.logical_not(stays))
    def _():
        received(r3, rs3)

    summed = r3[0].astype(F32)
    for j in range(1, 16):
        summed = summed + r3[j].astype(F32)

    ex = summed[:8, 1024:] + summed[8:, 1024:]
    factor = lax.rsqrt(ex[:, 16:17] * (1.0 / 2048) + EPS)
    ex = ex * factor
    summed = jnp.concatenate([summed[:8, :1024], summed[8:, :1024]], axis=1) * factor
    core0 = c == 0
    extra_log = dex[...].T
    queries, keys, values, gates, betas, rates = [], [], [], [], [], []
    for h in range(4):
        def head(m):
            return summed[:, 512 * m + 128 * h : 512 * m + 128 * (h + 1)]

        def unit(u):
            return u * lax.rsqrt(jnp.sum(u * u, axis=1, keepdims=True) + EPS)

        queries.append(unit(jax.nn.silu(head(0))) * 128 ** (-0.5))
        keys.append(unit(jax.nn.silu(head(1))))
        values.append(jax.nn.silu(head(2)))
        gates.append(jax.nn.silu(head(3)))
        betas.append(jax.nn.sigmoid(jnp.where(core0, ex[:, h : h + 1], ex[:, h + 4 : h + 5])))
        decay_in = jnp.where(core0, ex[:, h + 8 : h + 9], ex[:, h + 12 : h + 13])
        bias = jnp.where(core0, dib[:, h : h + 1], dib[:, h + 4 : h + 5])
        log_rate = jnp.where(core0, hdl[:, h : h + 1], hdl[:, h + 4 : h + 5])
        v = decay_in + bias
        softplus = jnp.maximum(v, 0.0) + jnp.log1p(jnp.exp(-jnp.abs(v)))
        rates.append(jnp.exp(extra_log[:, h : h + 1] - jnp.exp(log_rate) * softplus))
    columns = jnp.concatenate(keys + queries + [jnp.zeros((64, 128), F32)], axis=0).T
    for h in range(4):
        for s in range(8):
            m = 8 * h + s
            block = state[s, h]
            rec[h, pl.ds(s, 1), :] = jnp.sum(block * columns[:, m : m + 1], axis=0, keepdims=True)
            sq[h, pl.ds(s, 1), :] = jnp.sum(
                block * columns[:, 32 + m : 33 + m], axis=0, keepdims=True
            )
    heads, corrections = [], []
    for h in range(4):
        corr = betas[h] * (values[h] - rates[h] * rec[h])
        corrections.append(corr)
        key_query = jnp.sum(keys[h] * queries[h], axis=1, keepdims=True)
        read = rates[h] * sq[h] + key_query * corr
        norm = lax.rsqrt(jnp.sum(read * read, axis=1, keepdims=True) * (1.0 / 128) + EPS)
        heads.append(read * norm * hng[...] * gates[h])
    message = jnp.concatenate(
        [jnp.concatenate(heads[:2], axis=1), jnp.concatenate(heads[2:], axis=1)], axis=0
    ).astype(BF16)
    s4[...] = message

    slot = me % 8
    for n in range(15):
        remote(s4, r4.at[c, slot], ss4, rs4.at[c], chip_to(n), my_half).start()

    @pl.when(jnp.logical_not(stays))
    def _():
        remote(s4, r4.at[c, slot], ss4, rs4.at[c], me, other).start()

    @pl.when(stays)
    def _():
        r4[c, slot] = message

    for h in range(4):
        for s in range(8):
            m = 8 * h + s
            new_ref[s, h] = (
                state[s, h] * rates[h][s : s + 1, :]
                + columns[:, m : m + 1] * corrections[h][s : s + 1, :]
            )

    loaded(6, wo.at[c])
    shared(3, wo.at[other])

    @pl.when(stays)
    def _():
        received(r4.at[c, pl.ds(0, 7)], rs4.at[c])

    @pl.when(jnp.logical_not(stays))
    def _():
        received(r4.at[c], rs4.at[c])

    received(r4.at[other], rs4.at[other])
    mixer = jnp.zeros((64, 128), F32)
    for t in (0, 1):
        rows = []
        for i in range(8):
            part = r4[t, i].astype(F32)
            rows.append(jnp.concatenate([part[:8], part[8:]], axis=1))
        lhs = jnp.concatenate(rows, axis=0).astype(BF16)
        half = jnp.dot(lhs, wo[t], preferred_element_type=F32)
        mixer = mixer + half.astype(BF16).astype(F32)
    second = (first32 + mixer).astype(BF16)
    second32 = second.astype(F32)

    s5[...] = second
    for n in range(15):
        remote(s5, r5.at[n], ss5, rs5.at[group_of(n)], chip_to(n), c).start()

    def pack(block):
        upper, lower = block[:32], block[32:]
        return (
            jnp.where(low, upper, swap(lower)).astype(BF16),
            jnp.where(low, swap(upper), lower).astype(BF16),
        )

    p0, p1 = pack(second32)
    s7[0] = p0
    s7[1] = p1
    r7[c] = jnp.where(core0, p0, p1)
    remote(s7.at[other], r7.at[c], sp.at[1], rp.at[1], me, other).start()

    def arrived5(g):
        received(r5.at[group_slots(g)], rs5.at[g])

    def get5(n):
        if n == OWN:
            return second32
        return r5[n].astype(F32)

    loaded(7, w2.at[c])
    shared(4, w2.at[other])
    hidden2 = ffn_hidden(arrived5, get5, g2, w2)
    loaded(8, wd2.at[c])
    shared(5, wd2.at[other])

    def emit6(n, block):
        packs = pack(block)
        for t in (0, 1):
            s6[n, t] = packs[t]
        if n == OWN:
            r6[OWN, c] = jnp.where(core0, packs[0], packs[1])
            remote(s6.at[OWN, other], r6.at[OWN, c], sp.at[2], rp.at[2], me, other).start()
            return
        for t in (0, 1):
            remote(s6.at[n, t], r6.at[n, c], ss6, rs6.at[n // 8], chip_to(n), t).start()

    ffn_down(hidden2, wd2, emit6)

    sent(r1.at[pl.ds(0, 15)], ss1)
    sent(s1.at[0], sp.at[0])
    for i, ref in enumerate((w1, wd1, wp, wo, w2, wd2)):
        sent(ref.at[c], wsend_sem.at[i])
    sent(s2, ss2)

    @pl.when(stays)
    def _():
        sent(r3.at[pl.ds(0, 15)], ss3)
        sent(r6.at[pl.ds(0, 15), 0], ss4)

    @pl.when(jnp.logical_not(stays))
    def _():
        sent(r3, ss3)
        sent(r4, ss4)

    sent(r5, ss5)
    sent(s7.at[0], sp.at[1])

    received(r7.at[other], rp.at[1])
    received(r6.at[OWN, other], rp.at[2])
    totals = [r6[OWN, t].astype(F32) for t in (0, 1)]
    for n in range(14, -1, -1):
        if n == 14:
            received(r6.at[pl.ds(8, 7)], rs6.at[1])
        if n == 7:
            received(r6.at[pl.ds(0, 8)], rs6.at[0])
        for t in (0, 1):
            totals[t] = totals[t] + r6[n, t].astype(F32)
    rows = []
    for t in (0, 1):
        value = r7[t].astype(F32) + 0.5 * totals[t]
        rows += [value, swap(value)]
    out_ref[...] = jnp.concatenate(rows, axis=0).T[:64].astype(BF16)
    sent(r6.at[pl.ds(0, 15)], ss6)
    sent(s6.at[0, 0], sp.at[2])


def shards(
    tokens, first_norm_gain, first_gate_weight, first_up_weight, first_down_weight,
    mixer_norm_gain, query_weight, key_weight, value_weight, output_gate_weight,
    strength_weight, decay_weight, head_decay_log, decay_input_bias, decay_extra_log,
    head_norm_gain, state, mixer_output_weight,
    second_norm_gain, second_gate_weight, second_up_weight, second_down_weight,
):
    vm = pltpu.VMEM
    dma = pltpu.SemaphoreType.DMA
    scratch = [
        vm((64, 128), BF16), vm((16, 128), F32), vm((16, 128), F32), vm((16, 128), F32),
        vm((1, 8), F32), vm((1, 8), F32), vm((4, 8), F32), vm((1, 128), F32),
        vm((8, 128), BF16), vm((8, 128), BF16),
        vm((2, 2, 176, 2048), BF16), vm((2, 176, 2048), BF16),
        vm((2, 2, 176, 2048), BF16), vm((2, 176, 2048), BF16),
        vm((2, 128, 2048), BF16), vm((2, 512, 128), BF16), vm((8, 4, 128, 128), F32),
        vm((2, 32, 128), BF16), vm((16, 2, 32, 128), BF16),
        vm((15, 64, 128), BF16), vm((15, 64, 128), BF16),
        vm((2, 8, 16, 1152), BF16), vm((16, 16, 1152), BF16),
        vm((16, 256), BF16), vm((2, 8, 16, 256), BF16),
        vm((64, 128), BF16), vm((15, 64, 128), BF16),
        vm((16, 2, 32, 128), BF16), vm((16, 2, 32, 128), BF16),
        vm((2, 32, 128), BF16), vm((2, 32, 128), BF16),
        vm((4, 8, 128), F32), vm((4, 8, 128), F32),
        dma((17,)), dma((6,)), dma((6,)),
        dma, dma((4,)), dma, dma((2,)), dma, dma, dma, dma((2,)), dma, dma((4,)), dma, dma((2,)),
        dma((3,)), dma((3,)),
    ]
    out, new_state = pl.pallas_call(
        kernel,
        out_shape=(
            pltpu.VMEM((64, 128), BF16),
            pltpu.VMEM((8, 4, 128, 128), F32),
        ),
        in_specs=[pl.BlockSpec(memory_space=pltpu.HBM)] * 22,
        out_specs=[pl.BlockSpec(memory_space=pltpu.VMEM)] * 2,
        scratch_shapes=scratch,
        compiler_params=pltpu.CompilerParams(
            collective_id=0, has_side_effects=True, vmem_limit_bytes=64900000
        ),
        cost_estimate=pl.CostEstimate(
            flops=10**9, bytes_accessed=10**7, transcendentals=10**5
        ),
    )(
        tokens.T, first_norm_gain.reshape(16, 128), first_gate_weight.T, first_up_weight.T,
        first_down_weight, mixer_norm_gain.reshape(16, 128), query_weight, key_weight,
        value_weight, output_gate_weight, strength_weight.T, decay_weight.T,
        head_decay_log.reshape(1, 8), decay_input_bias.reshape(1, 8), decay_extra_log.T,
        head_norm_gain.reshape(1, 128), state, mixer_output_weight,
        second_norm_gain.reshape(16, 128), second_gate_weight.T, second_up_weight.T,
        second_down_weight,
    )
    return (out.T, new_state)


def solution(mesh):
    placed = (
        P("dp", ("kv", "tp")), P(), P(None, ("kv", "tp")), P(None, ("kv", "tp")),
        P(("kv", "tp"), None), P(), P("kv", "tp"), P("kv", "tp"), P("kv", "tp"),
        P("kv", "tp"), P(), P(), P(), P(), P(("dp", "kv"), "tp"), P(),
        P(("dp", "kv"), "tp", None, None), P("tp", "kv"), P(), P(None, ("kv", "tp")),
        P(None, ("kv", "tp")), P(("kv", "tp"), None),
    )
    return jax.shard_map(
        shards,
        mesh=mesh,
        in_specs=placed,
        out_specs=(P("dp", ("kv", "tp")), P(("dp", "kv"), "tp", None, None)),
        check_vma=False,
    )
```

```python
import jax
import jax.numpy as jnp
from jax import lax
from jax.experimental import pallas as pl
from jax.experimental.pallas import tpu as pltpu
from jax.sharding import PartitionSpec as P

EPS = 1e-06
F32 = jnp.float32
BF16 = jnp.bfloat16
MESH = pl.DeviceIdType.MESH
OFFSETS = sorted(
    [(a, b) for a in (0, 1, 2, 3) for b in (0, 1, 2, 3) if (a, b) != (0, 0)],
    key=lambda o: -(min(o[0], 4 - o[0]) + min(o[1], 4 - o[1])),
)
OWN = 15
ARRIVE = [OWN] + list(range(14, -1, -1))
ARRIVE_GROUPS = [ARRIVE[i : i + 4] for i in range(12, -1, -4)]


def group_of(n):
    return 3 if n == OWN else n // 4


def group_slots(g):
    return pl.ds(12, 3) if g == 3 else pl.ds(4 * g, 4)


SEND_GROUPS = [list(range(i, min(i + 4, 16))) for i in range(0, 16, 4)]


def kernel(
    tok_hbm, g1_hbm, wg1_hbm, wu1_hbm, wd1_hbm, gm_hbm,
    wq_hbm, wk_hbm, wv_hbm, wz_hbm, wstr_hbm, wdec_hbm,
    hdl_hbm, dib_hbm, dex_hbm, hng_hbm, state_hbm, wo_hbm,
    g2_hbm, wg2_hbm, wu2_hbm, wd2_hbm,
    out_ref, new_ref,
    tok, g1, gm, g2, hdl, dib, dex, hng, wstr, wdec,
    w1, wd1, w2, wd2, wp, wo, state,
    s1, r1, s2, r2, s3, r3, sx, rx, s4, r4, s5, r5, s6, r6, s7, r7,
    rec, sq,
    load_sem, wsend_sem, wrecv_sem,
    ss1, rs1, ss2, rs2, ss3, rs3, ssx, rsx, ss4, rs4, ss5, rs5, ss6, rs6, sp, rp,
):
    me = lax.axis_index("kv")
    c = lax.axis_index("tp")
    z = me // 4
    y = me % 4
    other = 1 - c
    my_half = me // 8

    def chip_to(n):
        a, b = OFFSETS[n] if n != OWN else (0, 0)
        return ((z + a) % 4) * 4 + (y + b) % 4

    def chip_from(n):
        a, b = OFFSETS[n] if n != OWN else (0, 0)
        return ((z + 4 - a) % 4) * 4 + (y + 4 - b) % 4

    def remote(src, dst, send, recv, chip, core):
        return pltpu.make_async_remote_copy(
            src_ref=src, dst_ref=dst, send_sem=send, recv_sem=recv,
            device_id={"kv": chip, "tp": core}, device_id_type=MESH,
        )

    def load(i, *pairs):
        for src, dst in pairs:
            pltpu.make_async_copy(src, dst, load_sem.at[i]).start()

    def loaded(i, ref):
        pltpu.make_async_copy(ref, ref, load_sem.at[i]).wait()

    rows_me = pl.ds(pl.multiple_of(me * 128, 128), 128)
    proj_src = (wq_hbm, wk_hbm, wv_hbm, wz_hbm)
    rows_c = pl.ds(pl.multiple_of(c * 176, 16), 176)
    rows_other = pl.ds(pl.multiple_of(other * 176, 16), 176)
    first_pairs = ((wg1_hbm, w1.at[0, rows_c]), (wu1_hbm, w1.at[1, rows_c]))
    second_pairs = ((wg2_hbm, w2.at[0, rows_c]), (wu2_hbm, w2.at[1, rows_c]))
    proj_pairs = tuple(
        (src, wp.at[c, :, pl.ds(512 * m, 512)]) for m, src in enumerate(proj_src)
    )
    load(0, (tok_hbm, tok))
    load(1, (g1_hbm, g1))
    load(2, *first_pairs)
    load(3, (wd1_hbm, wd1.at[rows_c]))
    small_pairs = (
        (gm_hbm, gm), (g2_hbm, g2), (hdl_hbm, hdl), (dib_hbm, dib), (dex_hbm, dex),
        (hng_hbm, hng), (wstr_hbm.at[:, rows_me], wstr), (wdec_hbm.at[:, rows_me], wdec),
    )
    for i, pair in enumerate(small_pairs):
        load(9 + i, pair)
    load(4, *proj_pairs)
    load(5, (state_hbm, state))
    load(6, (wo_hbm, wo.at[c]))
    load(7, *second_pairs)
    load(8, (wd2_hbm, wd2.at[rows_c]))

    barrier = pltpu.get_barrier_semaphore()
    for n in range(15):
        for t in (0, 1):
            pl.semaphore_signal(
                barrier, inc=1, device_id={"kv": chip_to(n), "tp": t}, device_id_type=MESH
            )
    pl.semaphore_signal(barrier, inc=1, device_id={"kv": me, "tp": other}, device_id_type=MESH)

    loaded(0, tok)
    packed = []
    all_rows = tok[...].astype(F32).T
    for t in (0, 1):
        rows = all_rows[64 * t : 64 * t + 64]
        packed.append(jnp.concatenate([rows[:32], rows[32:]], axis=1).astype(BF16))
        s1[t] = packed[t]
    r1[OWN, c] = jnp.where(c == 0, packed[0], packed[1])

    pl.semaphore_wait(barrier, 31)

    for n in range(15):
        for t in (0, 1):
            remote(
                s1.at[t], r1.at[n, c], ss1, rs1.at[group_of(n)], chip_to(n), t
            ).start()
    remote(s1.at[other], r1.at[OWN, c], sp.at[0], rp.at[0], me, other).start()

    def share(i, *pairs):
        for src, dst in pairs:
            remote(src, dst, wsend_sem.at[i], wrecv_sem.at[i], me, other).start()

    def shared(i, ref):
        remote(ref, ref, wsend_sem.at[i], wrecv_sem.at[i], me, other).wait_recv()

    def sent(ref, sem):
        remote(ref, ref, sem, rp.at[0], me, other).wait_send()

    def received(ref, sem):
        remote(ref, ref, sp.at[0], sem, me, other).wait_recv()

    share(0, *first_pairs)
    share(1, (wd1_hbm, wd1.at[rows_c]))
    share(2, *proj_pairs)

    lane = lax.broadcasted_iota(jnp.int32, (32, 128), 1)
    low = lane < 64

    def across(lhs, rhs):
        return lax.dot_general(
            lhs, rhs, (((1,), (1,)), ((), ())), preferred_element_type=F32
        )

    def swap(v):
        return pltpu.roll(v, 64, 1)

    def ffn_hidden(arrived, get, gain, w):
        squares = jnp.zeros((64, 128), F32)
        acc = None
        for g, group in enumerate(ARRIVE_GROUPS):
            arrived(g)
            parts, chips = [], []
            for n in group:
                x = get(n)
                j = chip_from(n)
                squares = squares + x * x
                parts.append((x * gain[pl.ds(j, 1), :]).astype(BF16))
                chips.append(j)
            lhs = jnp.concatenate(parts, axis=1)
            cols = [pl.ds(pl.multiple_of(j * 128, 128), 128) for j in chips]
            rhs = jnp.concatenate(
                [
                    jnp.concatenate([w[k, :, cs] for k in (0, 1)], axis=0)
                    for cs in cols
                ],
                axis=1,
            )
            d = across(lhs, rhs)
            acc = d if acc is None else acc + d
        scale = lax.rsqrt(jnp.sum(squares, axis=1, keepdims=True) * (1.0 / 2048) + EPS)
        gate = acc[:, :352] * scale
        return (jax.nn.silu(gate) * (acc[:, 352:] * scale)).astype(BF16)

    def ffn_down(hidden, w_down, emit):
        for group in SEND_GROUPS:
            cols = [pl.ds(pl.multiple_of(chip_to(n) * 128, 128), 128) for n in group]
            rhs = jnp.concatenate([w_down[:, cs] for cs in cols], axis=1)
            total = jnp.dot(hidden, rhs, preferred_element_type=F32)
            for i, n in enumerate(group):
                emit(n, total[:, 128 * i : 128 * (i + 1)])

    own_tokens = []

    def arrived1(g):
        if g == 3:
            received(r1.at[OWN, other], rp.at[0])
        received(r1.at[group_slots(g)], rs1.at[g])

    def get1(n):
        b0 = r1[n, 0].astype(F32)
        b1 = r1[n, 1].astype(F32)
        top = jnp.where(low, b0, swap(b1))
        bottom = jnp.where(low, swap(b0), b1)
        x = jnp.concatenate([top, bottom], axis=0)
        if n == OWN:
            own_tokens.append(x)
        return x

    loaded(1, g1)
    loaded(2, w1.at[:, rows_c])
    shared(0, w1.at[:, rows_other])
    hidden1 = ffn_hidden(arrived1, get1, g1, w1)

    loaded(3, wd1.at[rows_c])
    shared(1, wd1.at[rows_other])
    own2 = []

    def emit2(n, block):
        if n == OWN:
            own2.append(block)
            return
        s2[n] = block.astype(BF16)
        remote(s2.at[n], r2.at[n], ss2, rs2.at[n // 8], chip_to(n), c).start()

    ffn_down(hidden1, wd1, emit2)

    share(3, (wo_hbm, wo.at[c]))

    for i, (_, dst) in enumerate(small_pairs):
        loaded(9 + i, dst)
    loaded(4, wp.at[c])
    shared(2, wp.at[other])

    total = own2[0]
    for n in range(14, -1, -1):
        if n == 14:
            received(r2.at[pl.ds(8, 7)], rs2.at[1])
        if n == 7:
            received(r2.at[pl.ds(0, 8)], rs2.at[0])
        total = total + r2[n].astype(F32)
    first = (own_tokens[0] + 0.5 * total).astype(BF16)
    first32 = first.astype(F32)

    scaled = (first32 * gm[pl.ds(me, 1), :]).astype(BF16)
    strength = across(scaled, wstr[...])
    decay = across(scaled, wdec[...])
    sum_sq = jnp.sum(first32 * first32, axis=1, keepdims=True)
    extras = jnp.concatenate([strength, decay, sum_sq, jnp.zeros((64, 15), F32)], axis=1)
    extras_hi = extras.astype(BF16)
    extras_lo = (extras - extras_hi.astype(F32)).astype(BF16)
    extras = jnp.concatenate([extras_hi, extras_lo, jnp.zeros((64, 64), BF16)], axis=1)
    for i in range(8):
        sx[i] = extras[8 * i : 8 * i + 8]
    stays = c == my_half

    def to_owners(send, source_of, target, recv, own):
        for t in (0, 1):
            for k in range(8):
                i = (me + 5 + k) % 8
                chip = 8 * c + i
                is_self = jnp.logical_and(chip == me, c == t)

                @pl.when(jnp.logical_not(is_self))
                def _():
                    remote(source_of(t, i), target.at[me], send, recv, chip, t).start()

                @pl.when(is_self)
                def _():
                    target[me] = own(t, i)

    def from_owners(ref, sem):
        @pl.when(stays)
        def _():
            received(ref.at[pl.ds(0, 15)], sem)

        @pl.when(jnp.logical_not(stays))
        def _():
            received(ref, sem)

    for part in (0, 1):
        for t in (0, 1):
            proj = jnp.dot(
                scaled, wp[t, :, 1024 * part : 1024 * (part + 1)], preferred_element_type=F32
            )
            for i in range(8):
                rows = slice(8 * i, 8 * i + 8)
                s3[part, t, i] = jnp.concatenate(
                    [proj[rows, :512], proj[rows, 512:]], axis=0
                ).astype(BF16)
        to_owners(
            ss3.at[part],
            lambda t, i: s3.at[part, t, i],
            r3.at[part],
            rs3.at[part],
            lambda t, i: s3[part, t, i],
        )
        if part == 0:
            to_owners(ssx, lambda t, i: sx.at[i], rx, rsx, lambda t, i: sx[i])

    loaded(5, state)
    from_owners(r3.at[0], rs3.at[0])
    from_owners(rx, rsx)

    def summed_rows(ref):
        total = ref[0].astype(F32)
        for j in range(1, 16):
            total = total + ref[j].astype(F32)
        return total

    ex = summed_rows(rx)
    ex = ex + pltpu.roll(ex, 96, 1)
    factor = lax.rsqrt(ex[:, 16:17] * (1.0 / 2048) + EPS)
    ex = ex * factor
    summed = summed_rows(r3.at[0])
    core0 = c == 0
    extra_log = dex[...].T
    queries, keys, values, gates, betas, rates = [], [], [], [], [], []

    def unit(u):
        return u * lax.rsqrt(jnp.sum(u * u, axis=1, keepdims=True) + EPS)

    for h in range(4):
        lanes = slice(128 * h, 128 * (h + 1))
        queries.append(unit(jax.nn.silu(summed[:8, lanes] * factor)) * 128 ** (-0.5))
        keys.append(unit(jax.nn.silu(summed[8:, lanes] * factor)))
        betas.append(jax.nn.sigmoid(jnp.where(core0, ex[:, h : h + 1], ex[:, h + 4 : h + 5])))
        decay_in = jnp.where(core0, ex[:, h + 8 : h + 9], ex[:, h + 12 : h + 13])
        bias = jnp.where(core0, dib[:, h : h + 1], dib[:, h + 4 : h + 5])
        log_rate = jnp.where(core0, hdl[:, h : h + 1], hdl[:, h + 4 : h + 5])
        v = decay_in + bias
        softplus = jnp.maximum(v, 0.0) + jnp.log1p(jnp.exp(-jnp.abs(v)))
        rates.append(jnp.exp(extra_log[:, h : h + 1] - jnp.exp(log_rate) * softplus))
    columns = jnp.concatenate(keys + queries + [jnp.zeros((64, 128), F32)], axis=0).T
    for h in range(4):
        for s in range(8):
            m = 8 * h + s
            block = state[s, h]
            rec[h, pl.ds(s, 1), :] = jnp.sum(block * columns[:, m : m + 1], axis=0, keepdims=True)
            sq[h, pl.ds(s, 1), :] = jnp.sum(
                block * columns[:, 32 + m : 33 + m], axis=0, keepdims=True
            )
    from_owners(r3.at[1], rs3.at[1])
    summed = summed_rows(r3.at[1])
    for h in range(4):
        lanes = slice(128 * h, 128 * (h + 1))
        values.append(jax.nn.silu(summed[:8, lanes] * factor))
        gates.append(jax.nn.silu(summed[8:, lanes] * factor))
    heads, corrections = [], []
    for h in range(4):
        corr = betas[h] * (values[h] - rates[h] * rec[h])
        corrections.append(corr)
        key_query = jnp.sum(keys[h] * queries[h], axis=1, keepdims=True)
        read = rates[h] * sq[h] + key_query * corr
        norm = lax.rsqrt(jnp.sum(read * read, axis=1, keepdims=True) * (1.0 / 128) + EPS)
        heads.append(read * norm * hng[...] * gates[h])
    message = jnp.concatenate(
        [jnp.concatenate(heads[:2], axis=1), jnp.concatenate(heads[2:], axis=1)], axis=0
    ).astype(BF16)
    s4[...] = message

    slot = me % 8
    for n in range(15):
        remote(s4, r4.at[c, slot], ss4, rs4.at[c], chip_to(n), my_half).start()

    @pl.when(jnp.logical_not(stays))
    def _():
        remote(s4, r4.at[c, slot], ss4, rs4.at[c], me, other).start()

    @pl.when(stays)
    def _():
        r4[c, slot] = message

    share(4, *second_pairs)
    share(5, (wd2_hbm, wd2.at[rows_c]))

    for h in range(4):
        for s in range(8):
            m = 8 * h + s
            new_ref[s, h] = (
                state[s, h] * rates[h][s : s + 1, :]
                + columns[:, m : m + 1] * corrections[h][s : s + 1, :]
            )

    loaded(6, wo.at[c])
    shared(3, wo.at[other])

    @pl.when(stays)
    def _():
        received(r4.at[c, pl.ds(0, 7)], rs4.at[c])

    @pl.when(jnp.logical_not(stays))
    def _():
        received(r4.at[c], rs4.at[c])

    received(r4.at[other], rs4.at[other])
    mixer = jnp.zeros((64, 128), F32)
    for t in (0, 1):
        rows = []
        for i in range(8):
            part = r4[t, i].astype(F32)
            rows.append(jnp.concatenate([part[:8], part[8:]], axis=1))
        lhs = jnp.concatenate(rows, axis=0).astype(BF16)
        half = jnp.dot(lhs, wo[t], preferred_element_type=F32)
        mixer = mixer + half.astype(BF16).astype(F32)
    second = (first32 + mixer).astype(BF16)
    second32 = second.astype(F32)

    s5[...] = second
    for n in range(15):
        remote(s5, r5.at[n], ss5, rs5.at[group_of(n)], chip_to(n), c).start()

    def pack(block):
        upper, lower = block[:32], block[32:]
        return (
            jnp.where(low, upper, swap(lower)).astype(BF16),
            jnp.where(low, swap(upper), lower).astype(BF16),
        )

    p0, p1 = pack(second32)
    s7[0] = p0
    s7[1] = p1
    r7[c] = jnp.where(core0, p0, p1)
    remote(s7.at[other], r7.at[c], sp.at[1], rp.at[1], me, other).start()

    def arrived5(g):
        received(r5.at[group_slots(g)], rs5.at[g])

    def get5(n):
        if n == OWN:
            return second32
        return r5[n].astype(F32)

    loaded(7, w2.at[:, rows_c])
    shared(4, w2.at[:, rows_other])
    hidden2 = ffn_hidden(arrived5, get5, g2, w2)
    loaded(8, wd2.at[rows_c])
    shared(5, wd2.at[rows_other])

    def emit6(n, block):
        packs = pack(block)
        for t in (0, 1):
            s6[n, t] = packs[t]
        if n == OWN:
            r6[OWN, c] = jnp.where(core0, packs[0], packs[1])
            remote(s6.at[OWN, other], r6.at[OWN, c], sp.at[2], rp.at[2], me, other).start()
            return
        for t in (0, 1):
            remote(s6.at[n, t], r6.at[n, c], ss6, rs6.at[n // 8], chip_to(n), t).start()

    ffn_down(hidden2, wd2, emit6)

    sent(r1.at[pl.ds(0, 15)], ss1)
    sent(s1.at[0], sp.at[0])
    for i, ref in (
        (0, w1.at[:, rows_c]), (1, wd1.at[rows_c]), (2, wp.at[c]), (3, wo.at[c]),
        (4, w2.at[:, rows_c]), (5, wd2.at[rows_c]),
    ):
        sent(ref, wsend_sem.at[i])
    sent(s2, ss2)

    @pl.when(stays)
    def _():
        for part in (0, 1):
            sent(r3.at[part, pl.ds(0, 15)], ss3.at[part])
        sent(rx.at[pl.ds(0, 15)], ssx)
        sent(r6.at[pl.ds(0, 15), 0], ss4)

    @pl.when(jnp.logical_not(stays))
    def _():
        for part in (0, 1):
            sent(r3.at[part], ss3.at[part])
        sent(rx, ssx)
        sent(r4, ss4)

    sent(r5, ss5)
    sent(s7.at[0], sp.at[1])

    received(r7.at[other], rp.at[1])
    received(r6.at[OWN, other], rp.at[2])
    totals = [r6[OWN, t].astype(F32) for t in (0, 1)]
    for n in range(14, -1, -1):
        if n == 14:
            received(r6.at[pl.ds(8, 7)], rs6.at[1])
        if n == 7:
            received(r6.at[pl.ds(0, 8)], rs6.at[0])
        for t in (0, 1):
            totals[t] = totals[t] + r6[n, t].astype(F32)
    rows = []
    for t in (0, 1):
        value = r7[t].astype(F32) + 0.5 * totals[t]
        rows += [value, swap(value)]
    out_ref[...] = jnp.concatenate(rows, axis=0).T[:64].astype(BF16)
    sent(r6.at[pl.ds(0, 15)], ss6)
    sent(s6.at[0, 0], sp.at[2])


def shards(
    tokens, first_norm_gain, first_gate_weight, first_up_weight, first_down_weight,
    mixer_norm_gain, query_weight, key_weight, value_weight, output_gate_weight,
    strength_weight, decay_weight, head_decay_log, decay_input_bias, decay_extra_log,
    head_norm_gain, state, mixer_output_weight,
    second_norm_gain, second_gate_weight, second_up_weight, second_down_weight,
):
    vm = pltpu.VMEM
    dma = pltpu.SemaphoreType.DMA
    scratch = [
        vm((64, 128), BF16), vm((16, 128), F32), vm((16, 128), F32), vm((16, 128), F32),
        vm((1, 8), F32), vm((1, 8), F32), vm((4, 8), F32), vm((1, 128), F32),
        vm((8, 128), BF16), vm((8, 128), BF16),
        vm((2, 352, 2048), BF16), vm((352, 2048), BF16),
        vm((2, 352, 2048), BF16), vm((352, 2048), BF16),
        vm((2, 128, 2048), BF16), vm((2, 512, 128), BF16), vm((8, 4, 128, 128), F32),
        vm((2, 32, 128), BF16), vm((16, 2, 32, 128), BF16),
        vm((15, 64, 128), BF16), vm((15, 64, 128), BF16),
        vm((2, 2, 8, 16, 512), BF16), vm((2, 16, 16, 512), BF16),
        vm((8, 8, 128), BF16), vm((16, 8, 128), BF16),
        vm((16, 256), BF16), vm((2, 8, 16, 256), BF16),
        vm((64, 128), BF16), vm((15, 64, 128), BF16),
        vm((16, 2, 32, 128), BF16), vm((16, 2, 32, 128), BF16),
        vm((2, 32, 128), BF16), vm((2, 32, 128), BF16),
        vm((4, 8, 128), F32), vm((4, 8, 128), F32),
        dma((17,)), dma((6,)), dma((6,)),
        dma, dma((4,)), dma, dma((2,)), dma((2,)), dma((2,)), dma, dma, dma, dma((2,)), dma, dma((4,)), dma, dma((2,)),
        dma((3,)), dma((3,)),
    ]
    out, new_state = pl.pallas_call(
        kernel,
        out_shape=(
            pltpu.VMEM((64, 128), BF16),
            pltpu.VMEM((8, 4, 128, 128), F32),
        ),
        in_specs=[pl.BlockSpec(memory_space=pltpu.HBM)] * 22,
        out_specs=[pl.BlockSpec(memory_space=pltpu.VMEM)] * 2,
        scratch_shapes=scratch,
        compiler_params=pltpu.CompilerParams(
            collective_id=0, has_side_effects=True, vmem_limit_bytes=64900000
        ),
        cost_estimate=pl.CostEstimate(
            flops=10**9, bytes_accessed=10**7, transcendentals=10**5
        ),
    )(
        tokens.T, first_norm_gain.reshape(16, 128), first_gate_weight.T, first_up_weight.T,
        first_down_weight, mixer_norm_gain.reshape(16, 128), query_weight, key_weight,
        value_weight, output_gate_weight, strength_weight.T, decay_weight.T,
        head_decay_log.reshape(1, 8), decay_input_bias.reshape(1, 8), decay_extra_log.T,
        head_norm_gain.reshape(1, 128), state, mixer_output_weight,
        second_norm_gain.reshape(16, 128), second_gate_weight.T, second_up_weight.T,
        second_down_weight,
    )
    return (out.T, new_state)


def solution(mesh):
    placed = (
        P("dp", ("kv", "tp")), P(), P(None, ("kv", "tp")), P(None, ("kv", "tp")),
        P(("kv", "tp"), None), P(), P("kv", "tp"), P("kv", "tp"), P("kv", "tp"),
        P("kv", "tp"), P(), P(), P(), P(), P(("dp", "kv"), "tp"), P(),
        P(("dp", "kv"), "tp", None, None), P("tp", "kv"), P(), P(None, ("kv", "tp")),
        P(None, ("kv", "tp")), P(("kv", "tp"), None),
    )
    return jax.shard_map(
        shards,
        mesh=mesh,
        in_specs=placed,
        out_specs=(P("dp", ("kv", "tp")), P(("dp", "kv"), "tp", None, None)),
        check_vma=False,
    )
```

```python
import jax
import jax.numpy as jnp
from jax import lax
from jax.experimental import pallas as pl
from jax.experimental.pallas import tpu as pltpu
from jax.sharding import PartitionSpec as P

EPS = 1e-06
F32 = jnp.float32
BF16 = jnp.bfloat16
MESH = pl.DeviceIdType.MESH
OFFSETS = sorted(
    [(a, b) for a in (0, 1, 2, 3) for b in (0, 1, 2, 3) if (a, b) != (0, 0)],
    key=lambda o: -(min(o[0], 4 - o[0]) + min(o[1], 4 - o[1])),
)
OWN = 15
ARRIVE = [OWN] + list(range(14, -1, -1))
ARRIVE_GROUPS = [ARRIVE[i : i + 4] for i in range(12, -1, -4)]


def group_of(n):
    return 3 if n == OWN else n // 4


def group_slots(g):
    return pl.ds(12, 3) if g == 3 else pl.ds(4 * g, 4)


SEND_GROUPS = [list(range(i, min(i + 4, 16))) for i in range(0, 16, 4)]


def kernel(
    tok_hbm, g1_hbm, wg1_hbm, wu1_hbm, wd1_hbm, gm_hbm,
    wq_hbm, wk_hbm, wv_hbm, wz_hbm, wstr_hbm, wdec_hbm,
    hdl_hbm, dib_hbm, dex_hbm, hng_hbm, state_hbm, wo_hbm,
    g2_hbm, wg2_hbm, wu2_hbm, wd2_hbm,
    out_ref, new_ref,
    tok, g1, gm, g2, hdl, dib, dex, hng, wstr, wdec,
    w1, wd1, w2, wd2, wp, wo, state,
    s1, r1, s2, r2, s3, r3, sx, rx, s4, r4, s5, r5, s6, r6, s7, r7,
    stack,
    load_sem, wsend_sem, wrecv_sem,
    ss1, rs1, ss2, rs2, ss3, rs3, ssx, rsx, ss4, rs4, ss5, rs5, ss6, rs6, sp, rp,
):
    me = lax.axis_index("kv")
    c = lax.axis_index("tp")
    z = me // 4
    y = me % 4
    other = 1 - c
    my_half = me // 8

    def chip_to(n):
        a, b = OFFSETS[n] if n != OWN else (0, 0)
        return ((z + a) % 4) * 4 + (y + b) % 4

    def chip_from(n):
        a, b = OFFSETS[n] if n != OWN else (0, 0)
        return ((z + 4 - a) % 4) * 4 + (y + 4 - b) % 4

    def remote(src, dst, send, recv, chip, core):
        return pltpu.make_async_remote_copy(
            src_ref=src, dst_ref=dst, send_sem=send, recv_sem=recv,
            device_id={"kv": chip, "tp": core}, device_id_type=MESH,
        )

    def load(i, *pairs):
        for src, dst in pairs:
            pltpu.make_async_copy(src, dst, load_sem.at[i]).start()

    def loaded(i, ref):
        pltpu.make_async_copy(ref, ref, load_sem.at[i]).wait()

    rows_me = pl.ds(pl.multiple_of(me * 128, 128), 128)
    proj_src = (wq_hbm, wk_hbm, wv_hbm, wz_hbm)
    rows_c = pl.ds(pl.multiple_of(c * 176, 16), 176)
    rows_other = pl.ds(pl.multiple_of(other * 176, 16), 176)
    first_pairs = ((wg1_hbm, w1.at[0, rows_c]), (wu1_hbm, w1.at[1, rows_c]))
    second_pairs = ((wg2_hbm, w2.at[0, rows_c]), (wu2_hbm, w2.at[1, rows_c]))
    proj_pairs = tuple(
        (src, wp.at[c, :, pl.ds(512 * m, 512)]) for m, src in enumerate(proj_src)
    )
    load(0, (tok_hbm, tok))
    load(1, (g1_hbm, g1))
    load(2, *first_pairs)
    load(3, (wd1_hbm, wd1.at[rows_c]))
    small_pairs = (
        (gm_hbm, gm), (g2_hbm, g2), (hdl_hbm, hdl), (dib_hbm, dib), (dex_hbm, dex),
        (hng_hbm, hng), (wstr_hbm.at[:, rows_me], wstr), (wdec_hbm.at[:, rows_me], wdec),
    )
    for i, pair in enumerate(small_pairs):
        load(9 + i, pair)
    load(4, *proj_pairs)
    load(5, (state_hbm, state))
    load(6, (wo_hbm, wo.at[c]))
    load(7, *second_pairs)
    load(8, (wd2_hbm, wd2.at[rows_c]))

    barrier = pltpu.get_barrier_semaphore()
    for n in range(15):
        for t in (0, 1):
            pl.semaphore_signal(
                barrier, inc=1, device_id={"kv": chip_to(n), "tp": t}, device_id_type=MESH
            )
    pl.semaphore_signal(barrier, inc=1, device_id={"kv": me, "tp": other}, device_id_type=MESH)

    loaded(0, tok)
    packed = []
    all_rows = tok[...].astype(F32).T
    for t in (0, 1):
        rows = all_rows[64 * t : 64 * t + 64]
        packed.append(jnp.concatenate([rows[:32], rows[32:]], axis=1).astype(BF16))
        s1[t] = packed[t]
    r1[OWN, c] = jnp.where(c == 0, packed[0], packed[1])

    pl.semaphore_wait(barrier, 31)

    for n in range(15):
        for t in (0, 1):
            remote(
                s1.at[t], r1.at[n, c], ss1, rs1.at[group_of(n)], chip_to(n), t
            ).start()
    remote(s1.at[other], r1.at[OWN, c], sp.at[0], rp.at[0], me, other).start()

    def share(i, *pairs):
        for src, dst in pairs:
            remote(src, dst, wsend_sem.at[i], wrecv_sem.at[i], me, other).start()

    def shared(i, ref):
        remote(ref, ref, wsend_sem.at[i], wrecv_sem.at[i], me, other).wait_recv()

    def sent(ref, sem):
        remote(ref, ref, sem, rp.at[0], me, other).wait_send()

    def received(ref, sem):
        remote(ref, ref, sp.at[0], sem, me, other).wait_recv()

    share(0, *first_pairs)
    share(1, (wd1_hbm, wd1.at[rows_c]))
    share(2, *proj_pairs)

    lane = lax.broadcasted_iota(jnp.int32, (32, 128), 1)
    low = lane < 64

    def across(lhs, rhs):
        return lax.dot_general(
            lhs, rhs, (((1,), (1,)), ((), ())), preferred_element_type=F32
        )

    def swap(v):
        return pltpu.roll(v, 64, 1)

    def ffn_hidden(arrived, get, gain, w):
        squares = jnp.zeros((64, 128), F32)
        acc = None
        for g, group in enumerate(ARRIVE_GROUPS):
            arrived(g)
            parts, chips = [], []
            for n in group:
                x = get(n)
                j = chip_from(n)
                squares = squares + x * x
                parts.append((x * gain[pl.ds(j, 1), :]).astype(BF16))
                chips.append(j)
            lhs = jnp.concatenate(parts, axis=1)
            cols = [pl.ds(pl.multiple_of(j * 128, 128), 128) for j in chips]
            rhs = jnp.concatenate(
                [
                    jnp.concatenate([w[k, :, cs] for k in (0, 1)], axis=0)
                    for cs in cols
                ],
                axis=1,
            )
            d = across(lhs, rhs)
            acc = d if acc is None else acc + d
        scale = lax.rsqrt(jnp.sum(squares, axis=1, keepdims=True) * (1.0 / 2048) + EPS)
        gate = acc[:, :352] * scale
        return (jax.nn.silu(gate) * (acc[:, 352:] * scale)).astype(BF16)

    def ffn_down(hidden, w_down, emit):
        for group in SEND_GROUPS:
            cols = [pl.ds(pl.multiple_of(chip_to(n) * 128, 128), 128) for n in group]
            rhs = jnp.concatenate([w_down[:, cs] for cs in cols], axis=1)
            total = jnp.dot(hidden, rhs, preferred_element_type=F32)
            for i, n in enumerate(group):
                emit(n, total[:, 128 * i : 128 * (i + 1)])

    own_tokens = []

    def arrived1(g):
        if g == 3:
            received(r1.at[OWN, other], rp.at[0])
        received(r1.at[group_slots(g)], rs1.at[g])

    def get1(n):
        b0 = r1[n, 0].astype(F32)
        b1 = r1[n, 1].astype(F32)
        top = jnp.where(low, b0, swap(b1))
        bottom = jnp.where(low, swap(b0), b1)
        x = jnp.concatenate([top, bottom], axis=0)
        if n == OWN:
            own_tokens.append(x)
        return x

    loaded(1, g1)
    loaded(2, w1.at[:, rows_c])
    shared(0, w1.at[:, rows_other])
    hidden1 = ffn_hidden(arrived1, get1, g1, w1)

    loaded(3, wd1.at[rows_c])
    shared(1, wd1.at[rows_other])
    own2 = []

    def emit2(n, block):
        if n == OWN:
            own2.append(block)
            return
        s2[n] = block.astype(BF16)
        remote(s2.at[n], r2.at[n], ss2, rs2.at[n // 8], chip_to(n), c).start()

    ffn_down(hidden1, wd1, emit2)

    share(3, (wo_hbm, wo.at[c]))

    for i, (_, dst) in enumerate(small_pairs):
        loaded(9 + i, dst)
    loaded(4, wp.at[c])
    shared(2, wp.at[other])

    total = own2[0]
    for n in range(14, -1, -1):
        if n == 14:
            received(r2.at[pl.ds(8, 7)], rs2.at[1])
        if n == 7:
            received(r2.at[pl.ds(0, 8)], rs2.at[0])
        total = total + r2[n].astype(F32)
    first = (own_tokens[0] + 0.5 * total).astype(BF16)
    first32 = first.astype(F32)

    scaled = (first32 * gm[pl.ds(me, 1), :]).astype(BF16)
    strength = across(scaled, wstr[...])
    decay = across(scaled, wdec[...])
    sum_sq = jnp.sum(first32 * first32, axis=1, keepdims=True)
    extras = jnp.concatenate([strength, decay, sum_sq, jnp.zeros((64, 15), F32)], axis=1)
    extras_hi = extras.astype(BF16)
    extras_lo = (extras - extras_hi.astype(F32)).astype(BF16)
    extras = jnp.concatenate([extras_hi, extras_lo, jnp.zeros((64, 64), BF16)], axis=1)
    for i in range(8):
        sx[i] = extras[8 * i : 8 * i + 8]
    stays = c == my_half

    def to_owners(t, send, source_of, target, recv, own):
        for k in range(8):
            i = (me + 5 + k) % 8
            chip = 8 * c + i
            is_self = jnp.logical_and(chip == me, c == t)

            @pl.when(jnp.logical_not(is_self))
            def _():
                remote(source_of(i), target.at[me], send, recv, chip, t).start()

            @pl.when(is_self)
            def _():
                target[me] = own(i)

    def from_owners(ref, sem):
        @pl.when(stays)
        def _():
            received(ref.at[pl.ds(0, 15)], sem)

        @pl.when(jnp.logical_not(stays))
        def _():
            received(ref, sem)

    for part in (0, 1):
        for t in (0, 1):
            proj = jnp.dot(
                scaled, wp[t, :, 1024 * part : 1024 * (part + 1)], preferred_element_type=F32
            )
            for i in range(8):
                rows = slice(8 * i, 8 * i + 8)
                s3[part, t, i] = jnp.concatenate(
                    [proj[rows, :512], proj[rows, 512:]], axis=0
                ).astype(BF16)
            to_owners(
                t,
                ss3.at[part],
                lambda i: s3.at[part, t, i],
                r3.at[part],
                rs3.at[part],
                lambda i: s3[part, t, i],
            )
            if part == 0:
                to_owners(t, ssx, lambda i: sx.at[i], rx, rsx, lambda i: sx[i])

    loaded(5, state)
    for h in range(4):
        for s in range(8):
            stack[h // 2, 128 * s : 128 * (s + 1), 128 * (h % 2) : 128 * (h % 2 + 1)] = state[
                s, h
            ].astype(BF16)

    from_owners(r3.at[0], rs3.at[0])
    from_owners(rx, rsx)

    def summed_rows(ref):
        total = ref[0].astype(F32)
        for j in range(1, 16):
            total = total + ref[j].astype(F32)
        return total

    ex = summed_rows(rx)
    ex = ex + pltpu.roll(ex, 96, 1)
    factor = lax.rsqrt(ex[:, 16:17] * (1.0 / 2048) + EPS)
    ex = ex * factor
    summed = summed_rows(r3.at[0])
    core0 = c == 0
    extra_log = dex[...].T
    queries, keys, values, gates, betas, rates = [], [], [], [], [], []

    def unit(u):
        return u * lax.rsqrt(jnp.sum(u * u, axis=1, keepdims=True) + EPS)

    for h in range(4):
        lanes = slice(128 * h, 128 * (h + 1))
        queries.append(unit(jax.nn.silu(summed[:8, lanes] * factor)) * 128 ** (-0.5))
        keys.append(unit(jax.nn.silu(summed[8:, lanes] * factor)))
        betas.append(jax.nn.sigmoid(jnp.where(core0, ex[:, h : h + 1], ex[:, h + 4 : h + 5])))
        decay_in = jnp.where(core0, ex[:, h + 8 : h + 9], ex[:, h + 12 : h + 13])
        bias = jnp.where(core0, dib[:, h : h + 1], dib[:, h + 4 : h + 5])
        log_rate = jnp.where(core0, hdl[:, h : h + 1], hdl[:, h + 4 : h + 5])
        v = decay_in + bias
        softplus = jnp.maximum(v, 0.0) + jnp.log1p(jnp.exp(-jnp.abs(v)))
        rates.append(jnp.exp(extra_log[:, h : h + 1] - jnp.exp(log_rate) * softplus))
    row_seq = lax.broadcasted_iota(jnp.int32, (64, 128), 0) % 8
    recalls, reads = [], []
    for pair in (0, 1):
        rows = keys[2 * pair : 2 * pair + 2] + queries[2 * pair : 2 * pair + 2]
        rows = jnp.concatenate(rows, axis=0)
        high = rows.astype(BF16).astype(F32)
        rows = jnp.concatenate([high, rows - high], axis=0)
        lhs = jnp.concatenate(
            [jnp.where(row_seq == s, rows, 0.0) for s in range(8)], axis=1
        ).astype(BF16)
        both = jnp.dot(lhs, stack[pair], preferred_element_type=F32)
        both = both[:32] + both[32:]
        recalls += [both[:8, :128], both[8:16, 128:]]
        reads += [both[16:24, :128], both[24:, 128:]]
    from_owners(r3.at[1], rs3.at[1])
    summed = summed_rows(r3.at[1])
    for h in range(4):
        lanes = slice(128 * h, 128 * (h + 1))
        values.append(jax.nn.silu(summed[:8, lanes] * factor))
        gates.append(jax.nn.silu(summed[8:, lanes] * factor))
    heads, corrections = [], []
    for h in range(4):
        corr = betas[h] * (values[h] - rates[h] * recalls[h])
        corrections.append(corr)
        key_query = jnp.sum(keys[h] * queries[h], axis=1, keepdims=True)
        read = rates[h] * reads[h] + key_query * corr
        norm = lax.rsqrt(jnp.sum(read * read, axis=1, keepdims=True) * (1.0 / 128) + EPS)
        heads.append(read * norm * hng[...] * gates[h])
    message = jnp.concatenate(
        [jnp.concatenate(heads[:2], axis=1), jnp.concatenate(heads[2:], axis=1)], axis=0
    ).astype(BF16)
    s4[...] = message

    slot = me % 8
    for n in range(15):
        remote(s4, r4.at[c, slot], ss4, rs4.at[c], chip_to(n), my_half).start()

    @pl.when(jnp.logical_not(stays))
    def _():
        remote(s4, r4.at[c, slot], ss4, rs4.at[c], me, other).start()

    @pl.when(stays)
    def _():
        r4[c, slot] = message

    share(4, *second_pairs)
    share(5, (wd2_hbm, wd2.at[rows_c]))

    columns = jnp.concatenate(keys + [jnp.zeros((96, 128), F32)], axis=0).T
    for h in range(4):
        for s in range(8):
            m = 8 * h + s
            new_ref[s, h] = (
                state[s, h] * rates[h][s : s + 1, :]
                + columns[:, m : m + 1] * corrections[h][s : s + 1, :]
            )

    loaded(6, wo.at[c])
    shared(3, wo.at[other])

    @pl.when(stays)
    def _():
        received(r4.at[c, pl.ds(0, 7)], rs4.at[c])

    @pl.when(jnp.logical_not(stays))
    def _():
        received(r4.at[c], rs4.at[c])

    received(r4.at[other], rs4.at[other])
    mixer = jnp.zeros((64, 128), F32)
    for t in (0, 1):
        rows = []
        for i in range(8):
            part = r4[t, i].astype(F32)
            rows.append(jnp.concatenate([part[:8], part[8:]], axis=1))
        lhs = jnp.concatenate(rows, axis=0).astype(BF16)
        half = jnp.dot(lhs, wo[t], preferred_element_type=F32)
        mixer = mixer + half.astype(BF16).astype(F32)
    second = (first32 + mixer).astype(BF16)
    second32 = second.astype(F32)

    s5[...] = second
    for n in range(15):
        remote(s5, r5.at[n], ss5, rs5.at[group_of(n)], chip_to(n), c).start()

    def pack(block):
        upper, lower = block[:32], block[32:]
        return (
            jnp.where(low, upper, swap(lower)).astype(BF16),
            jnp.where(low, swap(upper), lower).astype(BF16),
        )

    p0, p1 = pack(second32)
    s7[0] = p0
    s7[1] = p1
    r7[c] = jnp.where(core0, p0, p1)
    remote(s7.at[other], r7.at[c], sp.at[1], rp.at[1], me, other).start()

    def arrived5(g):
        received(r5.at[group_slots(g)], rs5.at[g])

    def get5(n):
        if n == OWN:
            return second32
        return r5[n].astype(F32)

    loaded(7, w2.at[:, rows_c])
    shared(4, w2.at[:, rows_other])
    hidden2 = ffn_hidden(arrived5, get5, g2, w2)
    loaded(8, wd2.at[rows_c])
    shared(5, wd2.at[rows_other])

    def emit6(n, block):
        packs = pack(block)
        for t in (0, 1):
            s6[n, t] = packs[t]
        if n == OWN:
            r6[OWN, c] = jnp.where(core0, packs[0], packs[1])
            remote(s6.at[OWN, other], r6.at[OWN, c], sp.at[2], rp.at[2], me, other).start()
            return
        for t in (0, 1):
            remote(s6.at[n, t], r6.at[n, c], ss6, rs6.at[n // 8], chip_to(n), t).start()

    ffn_down(hidden2, wd2, emit6)

    sent(r1.at[pl.ds(0, 15)], ss1)
    sent(s1.at[0], sp.at[0])
    for i, ref in (
        (0, w1.at[:, rows_c]), (1, wd1.at[rows_c]), (2, wp.at[c]), (3, wo.at[c]),
        (4, w2.at[:, rows_c]), (5, wd2.at[rows_c]),
    ):
        sent(ref, wsend_sem.at[i])
    sent(s2, ss2)

    @pl.when(stays)
    def _():
        for part in (0, 1):
            sent(r3.at[part, pl.ds(0, 15)], ss3.at[part])
        sent(rx.at[pl.ds(0, 15)], ssx)
        sent(r6.at[pl.ds(0, 15), 0], ss4)

    @pl.when(jnp.logical_not(stays))
    def _():
        for part in (0, 1):
            sent(r3.at[part], ss3.at[part])
        sent(rx, ssx)
        sent(r4, ss4)

    sent(r5, ss5)
    sent(s7.at[0], sp.at[1])

    received(r7.at[other], rp.at[1])
    received(r6.at[OWN, other], rp.at[2])
    totals = [r6[OWN, t].astype(F32) for t in (0, 1)]
    for n in range(14, -1, -1):
        if n == 14:
            received(r6.at[pl.ds(8, 7)], rs6.at[1])
        if n == 7:
            received(r6.at[pl.ds(0, 8)], rs6.at[0])
        for t in (0, 1):
            totals[t] = totals[t] + r6[n, t].astype(F32)
    rows = []
    for t in (0, 1):
        value = r7[t].astype(F32) + 0.5 * totals[t]
        rows += [value, swap(value)]
    out_ref[...] = jnp.concatenate(rows, axis=0).T[:64].astype(BF16)
    sent(r6.at[pl.ds(0, 15)], ss6)
    sent(s6.at[0, 0], sp.at[2])


def write_out(out_ref, new_ref, out_hbm, new_hbm, sem):
    copies = [pltpu.make_async_copy(out_ref, out_hbm, sem.at[8])]
    copies += [pltpu.make_async_copy(new_ref.at[s], new_hbm.at[s], sem.at[s]) for s in range(8)]
    for copy in copies:
        copy.start()
    for copy in copies:
        copy.wait()


def shards(
    tokens, first_norm_gain, first_gate_weight, first_up_weight, first_down_weight,
    mixer_norm_gain, query_weight, key_weight, value_weight, output_gate_weight,
    strength_weight, decay_weight, head_decay_log, decay_input_bias, decay_extra_log,
    head_norm_gain, state, mixer_output_weight,
    second_norm_gain, second_gate_weight, second_up_weight, second_down_weight,
):
    vm = pltpu.VMEM
    dma = pltpu.SemaphoreType.DMA
    scratch = [
        vm((64, 128), BF16), vm((16, 128), F32), vm((16, 128), F32), vm((16, 128), F32),
        vm((1, 8), F32), vm((1, 8), F32), vm((4, 8), F32), vm((1, 128), F32),
        vm((8, 128), BF16), vm((8, 128), BF16),
        vm((2, 352, 2048), BF16), vm((352, 2048), BF16),
        vm((2, 352, 2048), BF16), vm((352, 2048), BF16),
        vm((2, 128, 2048), BF16), vm((2, 512, 128), BF16), vm((8, 4, 128, 128), F32),
        vm((2, 32, 128), BF16), vm((16, 2, 32, 128), BF16),
        vm((15, 64, 128), BF16), vm((15, 64, 128), BF16),
        vm((2, 2, 8, 16, 512), BF16), vm((2, 16, 16, 512), BF16),
        vm((8, 8, 128), BF16), vm((16, 8, 128), BF16),
        vm((16, 256), BF16), vm((2, 8, 16, 256), BF16),
        vm((64, 128), BF16), vm((15, 64, 128), BF16),
        vm((16, 2, 32, 128), BF16), vm((16, 2, 32, 128), BF16),
        vm((2, 32, 128), BF16), vm((2, 32, 128), BF16),
        vm((2, 1024, 256), BF16),
        dma((17,)), dma((6,)), dma((6,)),
        dma, dma((4,)), dma, dma((2,)), dma((2,)), dma((2,)), dma, dma, dma, dma((2,)), dma, dma((4,)), dma, dma((2,)),
        dma((3,)), dma((3,)),
    ]
    out, new_state = pl.pallas_call(
        kernel,
        out_shape=(
            pltpu.VMEM((64, 128), BF16),
            pltpu.VMEM((8, 4, 128, 128), F32),
        ),
        in_specs=[pl.BlockSpec(memory_space=pltpu.HBM)] * 22,
        out_specs=[pl.BlockSpec(memory_space=pltpu.VMEM)] * 2,
        scratch_shapes=scratch,
        compiler_params=pltpu.CompilerParams(
            collective_id=0, has_side_effects=True, vmem_limit_bytes=64900000
        ),
        cost_estimate=pl.CostEstimate(
            flops=10**9, bytes_accessed=10**7, transcendentals=10**5
        ),
    )(
        tokens.T, first_norm_gain.reshape(16, 128), first_gate_weight.T, first_up_weight.T,
        first_down_weight, mixer_norm_gain.reshape(16, 128), query_weight, key_weight,
        value_weight, output_gate_weight, strength_weight.T, decay_weight.T,
        head_decay_log.reshape(1, 8), decay_input_bias.reshape(1, 8), decay_extra_log.T,
        head_norm_gain.reshape(1, 128), state, mixer_output_weight,
        second_norm_gain.reshape(16, 128), second_gate_weight.T, second_up_weight.T,
        second_down_weight,
    )
    out, new_state = pl.pallas_call(
        write_out,
        out_shape=(
            jax.ShapeDtypeStruct((64, 128), BF16),
            jax.ShapeDtypeStruct((8, 4, 128, 128), F32),
        ),
        in_specs=[pl.BlockSpec(memory_space=pltpu.VMEM)] * 2,
        out_specs=[pl.BlockSpec(memory_space=pl.ANY)] * 2,
        scratch_shapes=[dma((9,))],
        compiler_params=pltpu.CompilerParams(vmem_limit_bytes=2**22),
    )(out, new_state)
    return (out.T, new_state)


def solution(mesh):
    placed = (
        P("dp", ("kv", "tp")), P(), P(None, ("kv", "tp")), P(None, ("kv", "tp")),
        P(("kv", "tp"), None), P(), P("kv", "tp"), P("kv", "tp"), P("kv", "tp"),
        P("kv", "tp"), P(), P(), P(), P(), P(("dp", "kv"), "tp"), P(),
        P(("dp", "kv"), "tp", None, None), P("tp", "kv"), P(), P(None, ("kv", "tp")),
        P(None, ("kv", "tp")), P(("kv", "tp"), None),
    )
    return jax.shard_map(
        shards,
        mesh=mesh,
        in_specs=placed,
        out_specs=(P("dp", ("kv", "tp")), P(("dp", "kv"), "tp", None, None)),
        check_vma=False,
    )
```

```python
import jax
import jax.numpy as jnp
from jax import lax
from jax.experimental import pallas as pl
from jax.experimental.pallas import tpu as pltpu
from jax.sharding import PartitionSpec as P

EPS = 1e-06
F32 = jnp.float32
BF16 = jnp.bfloat16
MESH = pl.DeviceIdType.MESH
OFFSETS = sorted(
    [(a, b) for a in (0, 1, 2, 3) for b in (0, 1, 2, 3) if (a, b) != (0, 0)],
    key=lambda o: -(min(o[0], 4 - o[0]) + min(o[1], 4 - o[1])),
)
OWN = 15
SEND_GROUPS = [list(range(i, min(i + 4, 16))) for i in range(0, 16, 4)]


def kernel(
    tok_hbm, g1_hbm, wg1_hbm, wu1_hbm, wd1_hbm, gm_hbm,
    wq_hbm, wk_hbm, wv_hbm, wz_hbm, wstr_hbm, wdec_hbm,
    hdl_hbm, dib_hbm, dex_hbm, hng_hbm, state_hbm, wo_hbm,
    g2_hbm, wg2_hbm, wu2_hbm, wd2_hbm,
    out_ref, new_ref,
    tok, g1, gm, g2, hdl, dib, dex, hng, wstr, wdec,
    w1, wd1, w2, wd2, wp, wo, state,
    s1, r1, s2, r2, s3, r3, sx, rx, s4, r4, s5, r5, s6, r6, s7, r7,
    stack,
    load_sem, wsend_sem, wrecv_sem,
    ss1, rs1, ss2, rs2, ss3, rs3, ssx, rsx, ss4, rs4, ss5, rs5, ss6, rs6, sp, rp,
):
    me = lax.axis_index("kv")
    c = lax.axis_index("tp")
    z = me // 4
    y = me % 4
    other = 1 - c
    my_half = me // 8

    def chip_to(n):
        a, b = OFFSETS[n] if n != OWN else (0, 0)
        return ((z + a) % 4) * 4 + (y + b) % 4

    def chip_from(n):
        a, b = OFFSETS[n] if n != OWN else (0, 0)
        return ((z + 4 - a) % 4) * 4 + (y + 4 - b) % 4

    def remote(src, dst, send, recv, chip, core):
        return pltpu.make_async_remote_copy(
            src_ref=src, dst_ref=dst, send_sem=send, recv_sem=recv,
            device_id={"kv": chip, "tp": core}, device_id_type=MESH,
        )

    def load(i, *pairs):
        for src, dst in pairs:
            pltpu.make_async_copy(src, dst, load_sem.at[i]).start()

    def loaded(i, ref):
        pltpu.make_async_copy(ref, ref, load_sem.at[i]).wait()

    rows_me = pl.ds(pl.multiple_of(me * 128, 128), 128)
    proj_src = (wq_hbm, wk_hbm, wv_hbm, wz_hbm)
    rows_c = pl.ds(pl.multiple_of(c * 176, 16), 176)
    rows_other = pl.ds(pl.multiple_of(other * 176, 16), 176)
    first_pairs = ((wg1_hbm, w1.at[0, rows_c]), (wu1_hbm, w1.at[1, rows_c]))
    second_pairs = ((wg2_hbm, w2.at[0, rows_c]), (wu2_hbm, w2.at[1, rows_c]))
    proj_pairs = tuple(
        (src, wp.at[c, :, pl.ds(512 * m, 512)]) for m, src in enumerate(proj_src)
    )
    load(0, (tok_hbm, tok))
    load(1, (g1_hbm, g1))
    load(2, *first_pairs)
    load(3, (wd1_hbm, wd1.at[rows_c]))
    small_pairs = (
        (gm_hbm, gm), (g2_hbm, g2), (hdl_hbm, hdl), (dib_hbm, dib), (dex_hbm, dex),
        (hng_hbm, hng), (wstr_hbm.at[:, rows_me], wstr), (wdec_hbm.at[:, rows_me], wdec),
    )
    for i, pair in enumerate(small_pairs):
        load(9 + i, pair)
    load(4, *proj_pairs)
    load(5, (state_hbm, state))
    load(6, (wo_hbm, wo.at[c]))
    load(7, *second_pairs)
    load(8, (wd2_hbm, wd2.at[rows_c]))

    barrier = pltpu.get_barrier_semaphore()
    for n in range(15):
        for t in (0, 1):
            pl.semaphore_signal(
                barrier, inc=1, device_id={"kv": chip_to(n), "tp": t}, device_id_type=MESH
            )
    pl.semaphore_signal(barrier, inc=1, device_id={"kv": me, "tp": other}, device_id_type=MESH)

    loaded(0, tok)
    packed = []
    all_rows = tok[...].astype(F32).T
    for t in (0, 1):
        rows = all_rows[64 * t : 64 * t + 64]
        packed.append(jnp.concatenate([rows[:32], rows[32:]], axis=1).astype(BF16))
        s1[t] = packed[t]
    r1[me, c] = jnp.where(c == 0, packed[0], packed[1])

    pl.semaphore_wait(barrier, 31)

    for n in range(15):
        for t in (0, 1):
            remote(
                s1.at[t], r1.at[me, c], ss1, rs1.at[z], chip_to(n), t
            ).start()
    remote(s1.at[other], r1.at[me, c], sp.at[0], rp.at[0], me, other).start()

    def share(i, *pairs):
        for src, dst in pairs:
            remote(src, dst, wsend_sem.at[i], wrecv_sem.at[i], me, other).start()

    def shared(i, ref):
        remote(ref, ref, wsend_sem.at[i], wrecv_sem.at[i], me, other).wait_recv()

    def sent(ref, sem):
        remote(ref, ref, sem, rp.at[0], me, other).wait_send()

    def received(ref, sem):
        remote(ref, ref, sp.at[0], sem, me, other).wait_recv()

    share(0, *first_pairs)
    share(1, (wd1_hbm, wd1.at[rows_c]))
    share(2, *proj_pairs)

    lane = lax.broadcasted_iota(jnp.int32, (32, 128), 1)
    low = lane < 64

    def across(lhs, rhs):
        return lax.dot_general(
            lhs, rhs, (((1,), (1,)), ((), ())), preferred_element_type=F32
        )

    def swap(v):
        return pltpu.roll(v, 64, 1)

    def ffn_hidden(order, arrived, get, gain, w):
        squares = jnp.zeros((64, 128), F32)
        acc = None
        for g in order:
            arrived(g)
            parts = []
            for j in range(4 * g, 4 * g + 4):
                x = get(j)
                squares = squares + x * x
                parts.append((x * gain[j : j + 1, :]).astype(BF16))
            lhs = jnp.concatenate(parts, axis=1)
            cs = slice(512 * g, 512 * (g + 1))
            rhs = jnp.concatenate([w[k, :, cs] for k in (0, 1)], axis=0)
            d = across(lhs, rhs)
            acc = d if acc is None else acc + d
        scale = lax.rsqrt(jnp.sum(squares, axis=1, keepdims=True) * (1.0 / 2048) + EPS)
        gate = acc[:, :352] * scale
        return (jax.nn.silu(gate) * (acc[:, 352:] * scale)).astype(BF16)

    def ffn_down(hidden, w_down, emit):
        for group in SEND_GROUPS:
            cols = [pl.ds(pl.multiple_of(chip_to(n) * 128, 128), 128) for n in group]
            rhs = jnp.concatenate([w_down[:, cs] for cs in cols], axis=1)
            total = jnp.dot(hidden, rhs, preferred_element_type=F32)
            for i, n in enumerate(group):
                emit(n, total[:, 128 * i : 128 * (i + 1)])

    def from_row(g, ref, sems):
        @pl.when(z == g)
        def _():
            received(ref.at[pl.ds(0, 3)], sems.at[g])

        @pl.when(z != g)
        def _():
            received(ref.at[pl.ds(0, 4)], sems.at[g])

    def arrived1(g):
        from_row(g, r1, rs1)

    def get1(n):
        b0 = r1[n, 0].astype(F32)
        b1 = r1[n, 1].astype(F32)
        top = jnp.where(low, b0, swap(b1))
        bottom = jnp.where(low, swap(b0), b1)
        x = jnp.concatenate([top, bottom], axis=0)
        return x

    loaded(1, g1)
    loaded(2, w1.at[:, rows_c])
    shared(0, w1.at[:, rows_other])
    received(r1.at[me, other], rp.at[0])
    hidden1 = ffn_hidden((2, 3, 1, 0), arrived1, get1, g1, w1)
    own_tokens = get1(me)

    loaded(3, wd1.at[rows_c])
    shared(1, wd1.at[rows_other])
    own2 = []

    def emit2(n, block):
        if n == OWN:
            own2.append(block)
            return
        s2[n] = block.astype(BF16)
        remote(s2.at[n], r2.at[n], ss2, rs2.at[n // 8], chip_to(n), c).start()

    ffn_down(hidden1, wd1, emit2)

    share(3, (wo_hbm, wo.at[c]))

    for i, (_, dst) in enumerate(small_pairs):
        loaded(9 + i, dst)
    loaded(4, wp.at[c])
    shared(2, wp.at[other])

    total = own2[0]
    for n in range(14, -1, -1):
        if n == 14:
            received(r2.at[pl.ds(8, 7)], rs2.at[1])
        if n == 7:
            received(r2.at[pl.ds(0, 8)], rs2.at[0])
        total = total + r2[n].astype(F32)
    first = (own_tokens + 0.5 * total).astype(BF16)
    first32 = first.astype(F32)

    scaled = (first32 * gm[pl.ds(me, 1), :]).astype(BF16)
    strength = across(scaled, wstr[...])
    decay = across(scaled, wdec[...])
    sum_sq = jnp.sum(first32 * first32, axis=1, keepdims=True)
    extras = jnp.concatenate([strength, decay, sum_sq, jnp.zeros((64, 15), F32)], axis=1)
    extras_hi = extras.astype(BF16)
    extras_lo = (extras - extras_hi.astype(F32)).astype(BF16)
    extras = jnp.concatenate([extras_hi, extras_lo, jnp.zeros((64, 64), BF16)], axis=1)
    for i in range(8):
        sx[i] = extras[8 * i : 8 * i + 8]
    stays = c == my_half

    def to_owners(t, send, source_of, target, recv, own):
        for k in range(8):
            i = (me + 5 + k) % 8
            chip = 8 * c + i
            is_self = jnp.logical_and(chip == me, c == t)

            @pl.when(jnp.logical_not(is_self))
            def _():
                remote(source_of(i), target.at[me], send, recv, chip, t).start()

            @pl.when(is_self)
            def _():
                target[me] = own(i)

    def from_owners(ref, sem):
        @pl.when(stays)
        def _():
            received(ref.at[pl.ds(0, 15)], sem)

        @pl.when(jnp.logical_not(stays))
        def _():
            received(ref, sem)

    for part in (0, 1):
        for t in (0, 1):
            proj = jnp.dot(
                scaled, wp[t, :, 1024 * part : 1024 * (part + 1)], preferred_element_type=F32
            )
            for i in range(8):
                rows = slice(8 * i, 8 * i + 8)
                s3[part, t, i] = jnp.concatenate(
                    [proj[rows, :512], proj[rows, 512:]], axis=0
                ).astype(BF16)
            to_owners(
                t,
                ss3.at[part],
                lambda i: s3.at[part, t, i],
                r3.at[part],
                rs3.at[part],
                lambda i: s3[part, t, i],
            )
            if part == 0:
                to_owners(t, ssx, lambda i: sx.at[i], rx, rsx, lambda i: sx[i])

    loaded(5, state)
    for h in range(4):
        for s in range(8):
            stack[h // 2, 128 * s : 128 * (s + 1), 128 * (h % 2) : 128 * (h % 2 + 1)] = state[
                s, h
            ].astype(BF16)

    from_owners(r3.at[0], rs3.at[0])
    from_owners(rx, rsx)

    def summed_rows(ref):
        total = ref[0].astype(F32)
        for j in range(1, 16):
            total = total + ref[j].astype(F32)
        return total

    ex = summed_rows(rx)
    ex = ex + pltpu.roll(ex, 96, 1)
    factor = lax.rsqrt(ex[:, 16:17] * (1.0 / 2048) + EPS)
    ex = ex * factor
    summed = summed_rows(r3.at[0])
    core0 = c == 0
    extra_log = dex[...].T
    queries, keys, values, gates, betas, rates = [], [], [], [], [], []

    def unit(u):
        return u * lax.rsqrt(jnp.sum(u * u, axis=1, keepdims=True) + EPS)

    for h in range(4):
        lanes = slice(128 * h, 128 * (h + 1))
        queries.append(unit(jax.nn.silu(summed[:8, lanes] * factor)) * 128 ** (-0.5))
        keys.append(unit(jax.nn.silu(summed[8:, lanes] * factor)))
        betas.append(jax.nn.sigmoid(jnp.where(core0, ex[:, h : h + 1], ex[:, h + 4 : h + 5])))
        decay_in = jnp.where(core0, ex[:, h + 8 : h + 9], ex[:, h + 12 : h + 13])
        bias = jnp.where(core0, dib[:, h : h + 1], dib[:, h + 4 : h + 5])
        log_rate = jnp.where(core0, hdl[:, h : h + 1], hdl[:, h + 4 : h + 5])
        v = decay_in + bias
        softplus = jnp.maximum(v, 0.0) + jnp.log1p(jnp.exp(-jnp.abs(v)))
        rates.append(jnp.exp(extra_log[:, h : h + 1] - jnp.exp(log_rate) * softplus))
    row_seq = lax.broadcasted_iota(jnp.int32, (64, 128), 0) % 8
    recalls, reads = [], []
    for pair in (0, 1):
        rows = keys[2 * pair : 2 * pair + 2] + queries[2 * pair : 2 * pair + 2]
        rows = jnp.concatenate(rows, axis=0)
        high = rows.astype(BF16).astype(F32)
        rows = jnp.concatenate([high, rows - high], axis=0)
        lhs = jnp.concatenate(
            [jnp.where(row_seq == s, rows, 0.0) for s in range(8)], axis=1
        ).astype(BF16)
        both = jnp.dot(lhs, stack[pair], preferred_element_type=F32)
        both = both[:32] + both[32:]
        recalls += [both[:8, :128], both[8:16, 128:]]
        reads += [both[16:24, :128], both[24:, 128:]]
    from_owners(r3.at[1], rs3.at[1])
    summed = summed_rows(r3.at[1])
    for h in range(4):
        lanes = slice(128 * h, 128 * (h + 1))
        values.append(jax.nn.silu(summed[:8, lanes] * factor))
        gates.append(jax.nn.silu(summed[8:, lanes] * factor))
    heads, corrections = [], []
    for h in range(4):
        corr = betas[h] * (values[h] - rates[h] * recalls[h])
        corrections.append(corr)
        key_query = jnp.sum(keys[h] * queries[h], axis=1, keepdims=True)
        read = rates[h] * reads[h] + key_query * corr
        norm = lax.rsqrt(jnp.sum(read * read, axis=1, keepdims=True) * (1.0 / 128) + EPS)
        heads.append(read * norm * hng[...] * gates[h])
    message = jnp.concatenate(
        [jnp.concatenate(heads[:2], axis=1), jnp.concatenate(heads[2:], axis=1)], axis=0
    ).astype(BF16)
    s4[...] = message

    slot = me % 8
    for n in range(15):
        remote(s4, r4.at[c, slot], ss4, rs4.at[c], chip_to(n), my_half).start()

    @pl.when(jnp.logical_not(stays))
    def _():
        remote(s4, r4.at[c, slot], ss4, rs4.at[c], me, other).start()

    @pl.when(stays)
    def _():
        r4[c, slot] = message

    share(4, *second_pairs)
    share(5, (wd2_hbm, wd2.at[rows_c]))

    columns = jnp.concatenate(keys + [jnp.zeros((96, 128), F32)], axis=0).T
    for h in range(4):
        for s in range(8):
            m = 8 * h + s
            new_ref[s, h] = (
                state[s, h] * rates[h][s : s + 1, :]
                + columns[:, m : m + 1] * corrections[h][s : s + 1, :]
            )

    loaded(6, wo.at[c])
    shared(3, wo.at[other])

    @pl.when(stays)
    def _():
        received(r4.at[c, pl.ds(0, 7)], rs4.at[c])

    @pl.when(jnp.logical_not(stays))
    def _():
        received(r4.at[c], rs4.at[c])

    received(r4.at[other], rs4.at[other])
    mixer = jnp.zeros((64, 128), F32)
    for t in (0, 1):
        rows = []
        for i in range(8):
            part = r4[t, i].astype(F32)
            rows.append(jnp.concatenate([part[:8], part[8:]], axis=1))
        lhs = jnp.concatenate(rows, axis=0).astype(BF16)
        half = jnp.dot(lhs, wo[t], preferred_element_type=F32)
        mixer = mixer + half.astype(BF16).astype(F32)
    second = (first32 + mixer).astype(BF16)
    second32 = second.astype(F32)

    s5[...] = second
    r5[me] = second
    for n in range(15):
        remote(s5, r5.at[me], ss5, rs5.at[z], chip_to(n), c).start()

    def pack(block):
        upper, lower = block[:32], block[32:]
        return (
            jnp.where(low, upper, swap(lower)).astype(BF16),
            jnp.where(low, swap(upper), lower).astype(BF16),
        )

    p0, p1 = pack(second32)
    s7[0] = p0
    s7[1] = p1
    r7[c] = jnp.where(core0, p0, p1)
    remote(s7.at[other], r7.at[c], sp.at[1], rp.at[1], me, other).start()

    def arrived5(g):
        from_row(g, r5, rs5)

    def get5(n):
        return r5[n].astype(F32)

    loaded(7, w2.at[:, rows_c])
    shared(4, w2.at[:, rows_other])
    hidden2 = ffn_hidden((1, 2, 0, 3), arrived5, get5, g2, w2)
    loaded(8, wd2.at[rows_c])
    shared(5, wd2.at[rows_other])

    def emit6(n, block):
        packs = pack(block)
        for t in (0, 1):
            s6[n, t] = packs[t]
        if n == OWN:
            r6[OWN, c] = jnp.where(core0, packs[0], packs[1])
            remote(s6.at[OWN, other], r6.at[OWN, c], sp.at[2], rp.at[2], me, other).start()
            return
        for t in (0, 1):
            remote(s6.at[n, t], r6.at[n, c], ss6, rs6.at[n // 8], chip_to(n), t).start()

    ffn_down(hidden2, wd2, emit6)

    sent(r1.at[pl.ds(0, 15)], ss1)
    sent(s1.at[0], sp.at[0])
    for i, ref in (
        (0, w1.at[:, rows_c]), (1, wd1.at[rows_c]), (2, wp.at[c]), (3, wo.at[c]),
        (4, w2.at[:, rows_c]), (5, wd2.at[rows_c]),
    ):
        sent(ref, wsend_sem.at[i])
    sent(s2, ss2)

    @pl.when(stays)
    def _():
        for part in (0, 1):
            sent(r3.at[part, pl.ds(0, 15)], ss3.at[part])
        sent(rx.at[pl.ds(0, 15)], ssx)
        sent(r6.at[pl.ds(0, 15), 0], ss4)

    @pl.when(jnp.logical_not(stays))
    def _():
        for part in (0, 1):
            sent(r3.at[part], ss3.at[part])
        sent(rx, ssx)
        sent(r4, ss4)

    sent(r5.at[pl.ds(0, 15)], ss5)
    sent(s7.at[0], sp.at[1])

    received(r7.at[other], rp.at[1])
    received(r6.at[OWN, other], rp.at[2])
    totals = [r6[OWN, t].astype(F32) for t in (0, 1)]
    for n in range(14, -1, -1):
        if n == 14:
            received(r6.at[pl.ds(8, 7)], rs6.at[1])
        if n == 7:
            received(r6.at[pl.ds(0, 8)], rs6.at[0])
        for t in (0, 1):
            totals[t] = totals[t] + r6[n, t].astype(F32)
    rows = []
    for t in (0, 1):
        value = r7[t].astype(F32) + 0.5 * totals[t]
        rows += [value, swap(value)]
    out_ref[...] = jnp.concatenate(rows, axis=0).T[:64].astype(BF16)
    sent(r6.at[pl.ds(0, 15)], ss6)
    sent(s6.at[0, 0], sp.at[2])


def write_out(out_ref, new_ref, out_hbm, new_hbm, sem):
    copies = [pltpu.make_async_copy(out_ref, out_hbm, sem.at[8])]
    copies += [pltpu.make_async_copy(new_ref.at[s], new_hbm.at[s], sem.at[s]) for s in range(8)]
    for copy in copies:
        copy.start()
    for copy in copies:
        copy.wait()


def shards(
    tokens, first_norm_gain, first_gate_weight, first_up_weight, first_down_weight,
    mixer_norm_gain, query_weight, key_weight, value_weight, output_gate_weight,
    strength_weight, decay_weight, head_decay_log, decay_input_bias, decay_extra_log,
    head_norm_gain, state, mixer_output_weight,
    second_norm_gain, second_gate_weight, second_up_weight, second_down_weight,
):
    vm = pltpu.VMEM
    dma = pltpu.SemaphoreType.DMA
    scratch = [
        vm((64, 128), BF16), vm((16, 128), F32), vm((16, 128), F32), vm((16, 128), F32),
        vm((1, 8), F32), vm((1, 8), F32), vm((4, 8), F32), vm((1, 128), F32),
        vm((8, 128), BF16), vm((8, 128), BF16),
        vm((2, 352, 2048), BF16), vm((352, 2048), BF16),
        vm((2, 352, 2048), BF16), vm((352, 2048), BF16),
        vm((2, 128, 2048), BF16), vm((2, 512, 128), BF16), vm((8, 4, 128, 128), F32),
        vm((2, 32, 128), BF16), vm((16, 2, 32, 128), BF16),
        vm((15, 64, 128), BF16), vm((15, 64, 128), BF16),
        vm((2, 2, 8, 16, 512), BF16), vm((2, 16, 16, 512), BF16),
        vm((8, 8, 128), BF16), vm((16, 8, 128), BF16),
        vm((16, 256), BF16), vm((2, 8, 16, 256), BF16),
        vm((64, 128), BF16), vm((16, 64, 128), BF16),
        vm((16, 2, 32, 128), BF16), vm((16, 2, 32, 128), BF16),
        vm((2, 32, 128), BF16), vm((2, 32, 128), BF16),
        vm((2, 1024, 256), BF16),
        dma((17,)), dma((6,)), dma((6,)),
        dma, dma((4,)), dma, dma((2,)), dma((2,)), dma((2,)), dma, dma, dma, dma((2,)), dma, dma((4,)), dma, dma((2,)),
        dma((3,)), dma((3,)),
    ]
    out, new_state = pl.pallas_call(
        kernel,
        out_shape=(
            pltpu.VMEM((64, 128), BF16),
            pltpu.VMEM((8, 4, 128, 128), F32),
        ),
        in_specs=[pl.BlockSpec(memory_space=pltpu.HBM)] * 22,
        out_specs=[pl.BlockSpec(memory_space=pltpu.VMEM)] * 2,
        scratch_shapes=scratch,
        compiler_params=pltpu.CompilerParams(
            collective_id=0, has_side_effects=True, vmem_limit_bytes=64900000
        ),
        cost_estimate=pl.CostEstimate(
            flops=10**9, bytes_accessed=10**7, transcendentals=10**5
        ),
    )(
        tokens.T, first_norm_gain.reshape(16, 128), first_gate_weight.T, first_up_weight.T,
        first_down_weight, mixer_norm_gain.reshape(16, 128), query_weight, key_weight,
        value_weight, output_gate_weight, strength_weight.T, decay_weight.T,
        head_decay_log.reshape(1, 8), decay_input_bias.reshape(1, 8), decay_extra_log.T,
        head_norm_gain.reshape(1, 128), state, mixer_output_weight,
        second_norm_gain.reshape(16, 128), second_gate_weight.T, second_up_weight.T,
        second_down_weight,
    )
    out, new_state = pl.pallas_call(
        write_out,
        out_shape=(
            jax.ShapeDtypeStruct((64, 128), BF16),
            jax.ShapeDtypeStruct((8, 4, 128, 128), F32),
        ),
        in_specs=[pl.BlockSpec(memory_space=pltpu.VMEM)] * 2,
        out_specs=[pl.BlockSpec(memory_space=pl.ANY)] * 2,
        scratch_shapes=[dma((9,))],
        compiler_params=pltpu.CompilerParams(vmem_limit_bytes=2**22),
    )(out, new_state)
    return (out.T, new_state)


def solution(mesh):
    placed = (
        P("dp", ("kv", "tp")), P(), P(None, ("kv", "tp")), P(None, ("kv", "tp")),
        P(("kv", "tp"), None), P(), P("kv", "tp"), P("kv", "tp"), P("kv", "tp"),
        P("kv", "tp"), P(), P(), P(), P(), P(("dp", "kv"), "tp"), P(),
        P(("dp", "kv"), "tp", None, None), P("tp", "kv"), P(), P(None, ("kv", "tp")),
        P(None, ("kv", "tp")), P(("kv", "tp"), None),
    )
    return jax.shard_map(
        shards,
        mesh=mesh,
        in_specs=placed,
        out_specs=(P("dp", ("kv", "tp")), P(("dp", "kv"), "tp", None, None)),
        check_vma=False,
    )
```

```python
import jax
import jax.numpy as jnp
from jax import lax
from jax.experimental import pallas as pl
from jax.experimental.pallas import tpu as pltpu
from jax.sharding import PartitionSpec as P

EPS = 1e-06
F32 = jnp.float32
BF16 = jnp.bfloat16
MESH = pl.DeviceIdType.MESH
OFFSETS = sorted(
    [(a, b) for a in (0, 1, 2, 3) for b in (0, 1, 2, 3) if (a, b) != (0, 0)],
    key=lambda o: -(min(o[0], 4 - o[0]) + min(o[1], 4 - o[1])),
)
OWN = 15
SEND_GROUPS = [list(range(i, min(i + 4, 16))) for i in range(0, 16, 4)]


def kernel(
    tok_hbm, g1_hbm, wg1_hbm, wu1_hbm, wd1_hbm, gm_hbm,
    wq_hbm, wk_hbm, wv_hbm, wz_hbm, wstr_hbm, wdec_hbm,
    hdl_hbm, dib_hbm, dex_hbm, hng_hbm, state_hbm, wo_hbm,
    g2_hbm, wg2_hbm, wu2_hbm, wd2_hbm,
    out_ref, new_ref,
    tok, g1, gm, g2, hdl, dib, dex, hng, wstr, wdec,
    w1, wd1, w2, wd2, wp, wo, state,
    s1, r1, s2, r2, s3, r3, sx, rx, s4, r4, s5, r5, s6, r6, s7, r7,
    stack,
    load_sem, wsend_sem, wrecv_sem,
    ss1, rs1, ss2, rs2, ss3, rs3, ssx, rsx, ss4, rs4, ss5, rs5, ss6, rs6, sp, rp,
):
    me = lax.axis_index("kv")
    c = lax.axis_index("tp")
    z = me // 4
    y = me % 4
    other = 1 - c
    my_half = me // 8

    def chip_to(n):
        a, b = OFFSETS[n] if n != OWN else (0, 0)
        return ((z + a) % 4) * 4 + (y + b) % 4

    def chip_from(n):
        a, b = OFFSETS[n] if n != OWN else (0, 0)
        return ((z + 4 - a) % 4) * 4 + (y + 4 - b) % 4

    def remote(src, dst, send, recv, chip, core):
        return pltpu.make_async_remote_copy(
            src_ref=src, dst_ref=dst, send_sem=send, recv_sem=recv,
            device_id={"kv": chip, "tp": core}, device_id_type=MESH,
        )

    def load(i, *pairs):
        for src, dst in pairs:
            pltpu.make_async_copy(src, dst, load_sem.at[i]).start()

    def loaded(i, ref):
        pltpu.make_async_copy(ref, ref, load_sem.at[i]).wait()

    rows_me = pl.ds(pl.multiple_of(me * 128, 128), 128)
    proj_src = (wq_hbm, wk_hbm, wv_hbm, wz_hbm)
    rows_c = pl.ds(pl.multiple_of(c * 176, 16), 176)
    rows_other = pl.ds(pl.multiple_of(other * 176, 16), 176)
    first_pairs = ((wg1_hbm, w1.at[0, rows_c]), (wu1_hbm, w1.at[1, rows_c]))
    second_pairs = ((wg2_hbm, w2.at[0, rows_c]), (wu2_hbm, w2.at[1, rows_c]))
    proj_pairs = tuple(
        (src, wp.at[c, :, pl.ds(512 * m, 512)]) for m, src in enumerate(proj_src)
    )
    load(0, (tok_hbm, tok))
    load(1, (g1_hbm, g1))
    load(2, *first_pairs)
    load(3, (wd1_hbm, wd1.at[rows_c]))
    small_pairs = (
        (gm_hbm, gm), (g2_hbm, g2), (hdl_hbm, hdl), (dib_hbm, dib), (dex_hbm, dex),
        (hng_hbm, hng), (wstr_hbm.at[:, rows_me], wstr), (wdec_hbm.at[:, rows_me], wdec),
    )
    for i, pair in enumerate(small_pairs):
        load(9 + i, pair)
    load(4, *proj_pairs)
    load(5, (state_hbm, state))
    load(6, (wo_hbm, wo.at[c]))
    load(7, *second_pairs)
    load(8, (wd2_hbm, wd2.at[rows_c]))

    barrier = pltpu.get_barrier_semaphore()
    for n in range(15):
        for t in (0, 1):
            pl.semaphore_signal(
                barrier, inc=1, device_id={"kv": chip_to(n), "tp": t}, device_id_type=MESH
            )
    pl.semaphore_signal(barrier, inc=1, device_id={"kv": me, "tp": other}, device_id_type=MESH)

    loaded(0, tok)
    packed = []
    all_rows = tok[...].astype(F32).T
    for t in (0, 1):
        rows = all_rows[64 * t : 64 * t + 64]
        packed.append(jnp.concatenate([rows[:32], rows[32:]], axis=1).astype(BF16))
        s1[t] = packed[t]
    r1[me, c] = jnp.where(c == 0, packed[0], packed[1])

    pl.semaphore_wait(barrier, 31)

    for n in range(15):
        for t in (0, 1):
            remote(
                s1.at[t], r1.at[me, c], ss1, rs1.at[z], chip_to(n), t
            ).start()
    remote(s1.at[other], r1.at[me, c], sp.at[0], rp.at[0], me, other).start()

    def share(i, *pairs):
        for src, dst in pairs:
            remote(src, dst, wsend_sem.at[i], wrecv_sem.at[i], me, other).start()

    def shared(i, ref):
        remote(ref, ref, wsend_sem.at[i], wrecv_sem.at[i], me, other).wait_recv()

    def sent(ref, sem):
        remote(ref, ref, sem, rp.at[0], me, other).wait_send()

    def received(ref, sem):
        remote(ref, ref, sp.at[0], sem, me, other).wait_recv()

    share(0, *first_pairs)
    share(1, (wd1_hbm, wd1.at[rows_c]))
    share(2, *proj_pairs)

    lane = lax.broadcasted_iota(jnp.int32, (32, 128), 1)
    low = lane < 64

    def across(lhs, rhs):
        return lax.dot_general(
            lhs, rhs, (((1,), (1,)), ((), ())), preferred_element_type=F32
        )

    def swap(v):
        return pltpu.roll(v, 64, 1)

    def ffn_hidden(order, arrived, get, gain, w):
        squares = jnp.zeros((64, 128), F32)
        acc = None
        for g in order:
            arrived(g)
            parts = []
            for j in range(4 * g, 4 * g + 4):
                x = get(j)
                squares = squares + x * x
                parts.append((x * gain[j : j + 1, :]).astype(BF16))
            lhs = jnp.concatenate(parts, axis=1)
            cs = slice(512 * g, 512 * (g + 1))
            rhs = jnp.concatenate([w[k, :, cs] for k in (0, 1)], axis=0)
            d = across(lhs, rhs)
            acc = d if acc is None else acc + d
        scale = lax.rsqrt(jnp.sum(squares, axis=1, keepdims=True) * (1.0 / 2048) + EPS)
        gate = acc[:, :352] * scale
        return (jax.nn.silu(gate) * (acc[:, 352:] * scale)).astype(BF16)

    def ffn_down(hidden, w_down, emit):
        for group in SEND_GROUPS:
            cols = [pl.ds(pl.multiple_of(chip_to(n) * 128, 128), 128) for n in group]
            rhs = jnp.concatenate([w_down[:, cs] for cs in cols], axis=1)
            total = jnp.dot(hidden, rhs, preferred_element_type=F32)
            for i, n in enumerate(group):
                emit(n, total[:, 128 * i : 128 * (i + 1)])

    def from_row(g, ref, sems):
        @pl.when(z == g)
        def _():
            received(ref.at[pl.ds(0, 3)], sems.at[g])

        @pl.when(z != g)
        def _():
            received(ref.at[pl.ds(0, 4)], sems.at[g])

    def arrived1(g):
        from_row(g, r1, rs1)

    def get1(n):
        b0 = r1[n, 0].astype(F32)
        b1 = r1[n, 1].astype(F32)
        top = jnp.where(low, b0, swap(b1))
        bottom = jnp.where(low, swap(b0), b1)
        x = jnp.concatenate([top, bottom], axis=0)
        return x

    loaded(1, g1)
    loaded(2, w1.at[:, rows_c])
    shared(0, w1.at[:, rows_other])
    received(r1.at[me, other], rp.at[0])
    hidden1 = ffn_hidden((2, 3, 1, 0), arrived1, get1, g1, w1)
    own_tokens = get1(me)

    loaded(3, wd1.at[rows_c])
    shared(1, wd1.at[rows_other])
    own2 = []

    def emit2(n, block):
        if n == OWN:
            own2.append(block)
            return
        s2[n] = block.astype(BF16)
        remote(s2.at[n], r2.at[n], ss2, rs2.at[n // 8], chip_to(n), c).start()

    ffn_down(hidden1, wd1, emit2)

    share(3, (wo_hbm, wo.at[c]))

    for i, (_, dst) in enumerate(small_pairs):
        loaded(9 + i, dst)
    loaded(4, wp.at[c])
    shared(2, wp.at[other])

    total = own2[0]
    for n in range(14, -1, -1):
        if n == 14:
            received(r2.at[pl.ds(8, 7)], rs2.at[1])
        if n == 7:
            received(r2.at[pl.ds(0, 8)], rs2.at[0])
        total = total + r2[n].astype(F32)
    first = (own_tokens + 0.5 * total).astype(BF16)
    first32 = first.astype(F32)

    scaled = (first32 * gm[pl.ds(me, 1), :]).astype(BF16)
    strength = across(scaled, wstr[...])
    decay = across(scaled, wdec[...])
    sum_sq = jnp.sum(first32 * first32, axis=1, keepdims=True)
    extras = jnp.concatenate([strength, decay, sum_sq, jnp.zeros((64, 15), F32)], axis=1)
    extras_hi = extras.astype(BF16)
    extras_lo = (extras - extras_hi.astype(F32)).astype(BF16)
    extras = jnp.concatenate([extras_hi, extras_lo, jnp.zeros((64, 64), BF16)], axis=1)
    for i in range(8):
        sx[i] = extras[8 * i : 8 * i + 8]
    stays = c == my_half

    def to_owners(t, send, source_of, target, recv, own):
        for k in range(8):
            i = (me + 5 + k) % 8
            chip = 8 * c + i
            is_self = jnp.logical_and(chip == me, c == t)

            @pl.when(jnp.logical_not(is_self))
            def _():
                remote(source_of(i), target.at[me], send, recv, chip, t).start()

            @pl.when(is_self)
            def _():
                target[me] = own(i)

    def from_owners(ref, sem):
        @pl.when(stays)
        def _():
            received(ref.at[pl.ds(0, 15)], sem)

        @pl.when(jnp.logical_not(stays))
        def _():
            received(ref, sem)

    for part in (0, 1):
        for t in (0, 1):
            proj = jnp.dot(
                scaled, wp[t, :, 1024 * part : 1024 * (part + 1)], preferred_element_type=F32
            )
            for i in range(8):
                rows = slice(8 * i, 8 * i + 8)
                s3[part, t, i] = jnp.concatenate(
                    [proj[rows, :512], proj[rows, 512:]], axis=0
                ).astype(BF16)
            to_owners(
                t,
                ss3.at[part],
                lambda i: s3.at[part, t, i],
                r3.at[part],
                rs3.at[part],
                lambda i: s3[part, t, i],
            )
            if part == 0:
                to_owners(t, ssx, lambda i: sx.at[i], rx, rsx, lambda i: sx[i])

    loaded(5, state)
    for h in range(4):
        for s in range(8):
            stack[h // 2, 128 * s : 128 * (s + 1), 128 * (h % 2) : 128 * (h % 2 + 1)] = state[
                s, h
            ].astype(BF16)

    from_owners(r3.at[0], rs3.at[0])
    from_owners(rx, rsx)

    def summed_rows(ref):
        total = ref[0].astype(F32)
        for j in range(1, 16):
            total = total + ref[j].astype(F32)
        return total

    ex = summed_rows(rx)
    ex = ex + pltpu.roll(ex, 96, 1)
    factor = lax.rsqrt(ex[:, 16:17] * (1.0 / 2048) + EPS)
    ex = ex * factor
    summed = summed_rows(r3.at[0])
    core0 = c == 0
    extra_log = dex[...].T
    queries, keys, values, gates, betas, rates = [], [], [], [], [], []

    def unit(u):
        return u * lax.rsqrt(jnp.sum(u * u, axis=1, keepdims=True) + EPS)

    for h in range(4):
        lanes = slice(128 * h, 128 * (h + 1))
        queries.append(unit(jax.nn.silu(summed[:8, lanes] * factor)) * 128 ** (-0.5))
        keys.append(unit(jax.nn.silu(summed[8:, lanes] * factor)))
        betas.append(jax.nn.sigmoid(jnp.where(core0, ex[:, h : h + 1], ex[:, h + 4 : h + 5])))
        decay_in = jnp.where(core0, ex[:, h + 8 : h + 9], ex[:, h + 12 : h + 13])
        bias = jnp.where(core0, dib[:, h : h + 1], dib[:, h + 4 : h + 5])
        log_rate = jnp.where(core0, hdl[:, h : h + 1], hdl[:, h + 4 : h + 5])
        v = decay_in + bias
        softplus = jnp.maximum(v, 0.0) + jnp.log1p(jnp.exp(-jnp.abs(v)))
        rates.append(jnp.exp(extra_log[:, h : h + 1] - jnp.exp(log_rate) * softplus))
    row_seq = lax.broadcasted_iota(jnp.int32, (64, 128), 0) % 8
    recalls, reads = [], []
    for pair in (0, 1):
        rows = keys[2 * pair : 2 * pair + 2] + queries[2 * pair : 2 * pair + 2]
        rows = jnp.concatenate(rows, axis=0)
        high = rows.astype(BF16).astype(F32)
        rows = jnp.concatenate([high, rows - high], axis=0)
        lhs = jnp.concatenate(
            [jnp.where(row_seq == s, rows, 0.0) for s in range(8)], axis=1
        ).astype(BF16)
        both = jnp.dot(lhs, stack[pair], preferred_element_type=F32)
        both = both[:32] + both[32:]
        recalls += [both[:8, :128], both[8:16, 128:]]
        reads += [both[16:24, :128], both[24:, 128:]]
    from_owners(r3.at[1], rs3.at[1])
    summed = summed_rows(r3.at[1])
    for h in range(4):
        lanes = slice(128 * h, 128 * (h + 1))
        values.append(jax.nn.silu(summed[:8, lanes] * factor))
        gates.append(jax.nn.silu(summed[8:, lanes] * factor))
    heads, corrections = [], []
    for h in range(4):
        corr = betas[h] * (values[h] - rates[h] * recalls[h])
        corrections.append(corr)
        key_query = jnp.sum(keys[h] * queries[h], axis=1, keepdims=True)
        read = rates[h] * reads[h] + key_query * corr
        norm = lax.rsqrt(jnp.sum(read * read, axis=1, keepdims=True) * (1.0 / 128) + EPS)
        heads.append(read * norm * hng[...] * gates[h])
    message = jnp.concatenate(
        [jnp.concatenate(heads[:2], axis=1), jnp.concatenate(heads[2:], axis=1)], axis=0
    ).astype(BF16)
    s4[...] = message

    slot = me % 8
    for n in range(15):
        remote(s4, r4.at[c, slot], ss4, rs4.at[c], chip_to(n), my_half).start()

    @pl.when(jnp.logical_not(stays))
    def _():
        remote(s4, r4.at[c, slot], ss4, rs4.at[c], me, other).start()

    @pl.when(stays)
    def _():
        r4[c, slot] = message

    share(4, *second_pairs)
    share(5, (wd2_hbm, wd2.at[rows_c]))

    columns = jnp.concatenate(keys + [jnp.zeros((96, 128), F32)], axis=0).T
    for h in range(4):
        for s in range(8):
            m = 8 * h + s
            new_ref[s, h] = (
                state[s, h] * rates[h][s : s + 1, :]
                + columns[:, m : m + 1] * corrections[h][s : s + 1, :]
            )

    loaded(6, wo.at[c])
    shared(3, wo.at[other])

    @pl.when(stays)
    def _():
        received(r4.at[c, pl.ds(0, 7)], rs4.at[c])

    @pl.when(jnp.logical_not(stays))
    def _():
        received(r4.at[c], rs4.at[c])

    received(r4.at[other], rs4.at[other])
    mixer = jnp.zeros((64, 128), F32)
    for t in (0, 1):
        rows = []
        for i in range(8):
            part = r4[t, i].astype(F32)
            rows.append(jnp.concatenate([part[:8], part[8:]], axis=1))
        lhs = jnp.concatenate(rows, axis=0).astype(BF16)
        half = jnp.dot(lhs, wo[t], preferred_element_type=F32)
        mixer = mixer + half.astype(BF16).astype(F32)
    second = (first32 + mixer).astype(BF16)
    second32 = second.astype(F32)

    s5[...] = second
    r5[me] = second
    for n in range(15):
        remote(s5, r5.at[me], ss5, rs5.at[z], chip_to(n), c).start()

    def pack(block):
        upper, lower = block[:32], block[32:]
        return (
            jnp.where(low, upper, swap(lower)).astype(BF16),
            jnp.where(low, swap(upper), lower).astype(BF16),
        )

    p0, p1 = pack(second32)
    s7[0] = p0
    s7[1] = p1
    r7[c] = jnp.where(core0, p0, p1)
    remote(s7.at[other], r7.at[c], sp.at[1], rp.at[1], me, other).start()

    def arrived5(g):
        from_row(g, r5, rs5)

    def get5(n):
        return r5[n].astype(F32)

    loaded(7, w2.at[:, rows_c])
    shared(4, w2.at[:, rows_other])
    hidden2 = ffn_hidden((1, 2, 0, 3), arrived5, get5, g2, w2)
    loaded(8, wd2.at[rows_c])
    shared(5, wd2.at[rows_other])

    def emit6(n, block):
        packs = pack(block)
        for t in (0, 1):
            s6[n, t] = packs[t]
        if n == OWN:
            r6[OWN, c] = jnp.where(core0, packs[0], packs[1])
            remote(s6.at[OWN, other], r6.at[OWN, c], sp.at[2], rp.at[2], me, other).start()
            return
        for t in (0, 1):
            remote(s6.at[n, t], r6.at[n, c], ss6, rs6.at[n // 8], chip_to(n), t).start()

    ffn_down(hidden2, wd2, emit6)

    received(r7.at[other], rp.at[1])
    received(r6.at[OWN, other], rp.at[2])
    totals = [r6[OWN, t].astype(F32) for t in (0, 1)]
    for n in range(14, -1, -1):
        if n == 14:
            received(r6.at[pl.ds(8, 7)], rs6.at[1])
        if n == 7:
            received(r6.at[pl.ds(0, 8)], rs6.at[0])
        for t in (0, 1):
            totals[t] = totals[t] + r6[n, t].astype(F32)
    rows = []
    for t in (0, 1):
        value = r7[t].astype(F32) + 0.5 * totals[t]
        rows += [value, swap(value)]
    out_ref[...] = jnp.concatenate(rows, axis=0).T[:64].astype(BF16)
    sent(r1.at[pl.ds(0, 15)], ss1)
    sent(s1.at[0], sp.at[0])
    for i, ref in (
        (0, w1.at[:, rows_c]), (1, wd1.at[rows_c]), (2, wp.at[c]), (3, wo.at[c]),
        (4, w2.at[:, rows_c]), (5, wd2.at[rows_c]),
    ):
        sent(ref, wsend_sem.at[i])
    sent(s2, ss2)

    @pl.when(stays)
    def _():
        for part in (0, 1):
            sent(r3.at[part, pl.ds(0, 15)], ss3.at[part])
        sent(rx.at[pl.ds(0, 15)], ssx)
        sent(r6.at[pl.ds(0, 15), 0], ss4)

    @pl.when(jnp.logical_not(stays))
    def _():
        for part in (0, 1):
            sent(r3.at[part], ss3.at[part])
        sent(rx, ssx)
        sent(r4, ss4)

    sent(r5.at[pl.ds(0, 15)], ss5)
    sent(s7.at[0], sp.at[1])

    sent(r6.at[pl.ds(0, 15)], ss6)
    sent(s6.at[0, 0], sp.at[2])


def write_out(out_ref, new_ref, out_hbm, new_hbm, sem):
    copies = [pltpu.make_async_copy(out_ref, out_hbm, sem.at[8])]
    copies += [pltpu.make_async_copy(new_ref.at[s], new_hbm.at[s], sem.at[s]) for s in range(8)]
    for copy in copies:
        copy.start()
    for copy in copies:
        copy.wait()


def shards(
    tokens, first_norm_gain, first_gate_weight, first_up_weight, first_down_weight,
    mixer_norm_gain, query_weight, key_weight, value_weight, output_gate_weight,
    strength_weight, decay_weight, head_decay_log, decay_input_bias, decay_extra_log,
    head_norm_gain, state, mixer_output_weight,
    second_norm_gain, second_gate_weight, second_up_weight, second_down_weight,
):
    vm = pltpu.VMEM
    dma = pltpu.SemaphoreType.DMA
    scratch = [
        vm((64, 128), BF16), vm((16, 128), F32), vm((16, 128), F32), vm((16, 128), F32),
        vm((1, 8), F32), vm((1, 8), F32), vm((4, 8), F32), vm((1, 128), F32),
        vm((8, 128), BF16), vm((8, 128), BF16),
        vm((2, 352, 2048), BF16), vm((352, 2048), BF16),
        vm((2, 352, 2048), BF16), vm((352, 2048), BF16),
        vm((2, 128, 2048), BF16), vm((2, 512, 128), BF16), vm((8, 4, 128, 128), F32),
        vm((2, 32, 128), BF16), vm((16, 2, 32, 128), BF16),
        vm((15, 64, 128), BF16), vm((15, 64, 128), BF16),
        vm((2, 2, 8, 16, 512), BF16), vm((2, 16, 16, 512), BF16),
        vm((8, 8, 128), BF16), vm((16, 8, 128), BF16),
        vm((16, 256), BF16), vm((2, 8, 16, 256), BF16),
        vm((64, 128), BF16), vm((16, 64, 128), BF16),
        vm((16, 2, 32, 128), BF16), vm((16, 2, 32, 128), BF16),
        vm((2, 32, 128), BF16), vm((2, 32, 128), BF16),
        vm((2, 1024, 256), BF16),
        dma((17,)), dma((6,)), dma((6,)),
        dma, dma((4,)), dma, dma((2,)), dma((2,)), dma((2,)), dma, dma, dma, dma((2,)), dma, dma((4,)), dma, dma((2,)),
        dma((3,)), dma((3,)),
    ]
    out, new_state = pl.pallas_call(
        kernel,
        out_shape=(
            pltpu.VMEM((64, 128), BF16),
            pltpu.VMEM((8, 4, 128, 128), F32),
        ),
        in_specs=[pl.BlockSpec(memory_space=pltpu.HBM)] * 22,
        out_specs=[pl.BlockSpec(memory_space=pltpu.VMEM)] * 2,
        scratch_shapes=scratch,
        compiler_params=pltpu.CompilerParams(
            collective_id=0, has_side_effects=True, vmem_limit_bytes=64900000
        ),
        cost_estimate=pl.CostEstimate(
            flops=10**9, bytes_accessed=10**7, transcendentals=10**5
        ),
    )(
        tokens.T, first_norm_gain.reshape(16, 128), first_gate_weight.T, first_up_weight.T,
        first_down_weight, mixer_norm_gain.reshape(16, 128), query_weight, key_weight,
        value_weight, output_gate_weight, strength_weight.T, decay_weight.T,
        head_decay_log.reshape(1, 8), decay_input_bias.reshape(1, 8), decay_extra_log.T,
        head_norm_gain.reshape(1, 128), state, mixer_output_weight,
        second_norm_gain.reshape(16, 128), second_gate_weight.T, second_up_weight.T,
        second_down_weight,
    )
    out, new_state = pl.pallas_call(
        write_out,
        out_shape=(
            jax.ShapeDtypeStruct((64, 128), BF16),
            jax.ShapeDtypeStruct((8, 4, 128, 128), F32),
        ),
        in_specs=[pl.BlockSpec(memory_space=pltpu.VMEM)] * 2,
        out_specs=[pl.BlockSpec(memory_space=pl.ANY)] * 2,
        scratch_shapes=[dma((9,))],
        compiler_params=pltpu.CompilerParams(vmem_limit_bytes=2**22),
    )(out, new_state)
    return (out.T, new_state)


def solution(mesh):
    placed = (
        P("dp", ("kv", "tp")), P(), P(None, ("kv", "tp")), P(None, ("kv", "tp")),
        P(("kv", "tp"), None), P(), P("kv", "tp"), P("kv", "tp"), P("kv", "tp"),
        P("kv", "tp"), P(), P(), P(), P(), P(("dp", "kv"), "tp"), P(),
        P(("dp", "kv"), "tp", None, None), P("tp", "kv"), P(), P(None, ("kv", "tp")),
        P(None, ("kv", "tp")), P(("kv", "tp"), None),
    )
    return jax.shard_map(
        shards,
        mesh=mesh,
        in_specs=placed,
        out_specs=(P("dp", ("kv", "tp")), P(("dp", "kv"), "tp", None, None)),
        check_vma=False,
    )
```

```python
import jax
import jax.numpy as jnp
from jax import lax
from jax.experimental import pallas as pl
from jax.experimental.pallas import tpu as pltpu
from jax.sharding import PartitionSpec as P

EPS = 1e-06
F32 = jnp.float32
BF16 = jnp.bfloat16
MESH = pl.DeviceIdType.MESH
OFFSETS = sorted(
    [(a, b) for a in (0, 1, 2, 3) for b in (0, 1, 2, 3) if (a, b) != (0, 0)],
    key=lambda o: -(min(o[0], 4 - o[0]) + min(o[1], 4 - o[1])),
)
OWN = 15
SEND_GROUPS = [list(range(i, min(i + 4, 16))) for i in range(0, 16, 4)]


def kernel(
    tok_hbm, g1_hbm, wg1_hbm, wu1_hbm, wd1_hbm, gm_hbm,
    wq_hbm, wk_hbm, wv_hbm, wz_hbm, wstr_hbm, wdec_hbm,
    hdl_hbm, dib_hbm, dex_hbm, hng_hbm, state_hbm, wo_hbm,
    g2_hbm, wg2_hbm, wu2_hbm, wd2_hbm,
    out_ref, new_ref,
    tok, g1, gm, g2, hdl, dib, dex, hng, wstr, wdec,
    w1, wd1, w2, wd2, wp, wo, state,
    s1, r1, s2, r2, s3, r3, sx, rx, s4, r4, s5, r5, s6, r6, s7, r7,
    stack,
    load_sem, wsend_sem, wrecv_sem,
    ss1, rs1, ss2, rs2, ss3, rs3, ssx, rsx, ss4, rs4, ss5, rs5, ss6, rs6, sp, rp,
):
    me = lax.axis_index("kv")
    c = lax.axis_index("tp")
    z = me // 4
    y = me % 4
    other = 1 - c
    my_half = me // 8

    def chip_to(n):
        a, b = OFFSETS[n] if n != OWN else (0, 0)
        return ((z + a) % 4) * 4 + (y + b) % 4

    def chip_from(n):
        a, b = OFFSETS[n] if n != OWN else (0, 0)
        return ((z + 4 - a) % 4) * 4 + (y + 4 - b) % 4

    def remote(src, dst, send, recv, chip, core):
        return pltpu.make_async_remote_copy(
            src_ref=src, dst_ref=dst, send_sem=send, recv_sem=recv,
            device_id={"kv": chip, "tp": core}, device_id_type=MESH,
        )

    pltpu.make_async_copy(tok_hbm, tok, load_sem.at[0]).start()

    barrier = pltpu.get_barrier_semaphore()
    for n in range(15):
        for t in (0, 1):
            pl.semaphore_signal(
                barrier, inc=1, device_id={"kv": chip_to(n), "tp": t}, device_id_type=MESH
            )
    pl.semaphore_signal(barrier, inc=1, device_id={"kv": me, "tp": other}, device_id_type=MESH)

    def load(i, *pairs):
        for src, dst in pairs:
            pltpu.make_async_copy(src, dst, load_sem.at[i]).start()

    def loaded(i, ref):
        pltpu.make_async_copy(ref, ref, load_sem.at[i]).wait()

    rows_me = pl.ds(pl.multiple_of(me * 128, 128), 128)
    proj_src = (wq_hbm, wk_hbm, wv_hbm, wz_hbm)
    rows_c = pl.ds(pl.multiple_of(c * 176, 16), 176)
    rows_other = pl.ds(pl.multiple_of(other * 176, 16), 176)
    first_pairs = ((wg1_hbm, w1.at[0, rows_c]), (wu1_hbm, w1.at[1, rows_c]))
    second_pairs = ((wg2_hbm, w2.at[0, rows_c]), (wu2_hbm, w2.at[1, rows_c]))
    proj_pairs = tuple(
        (src, wp.at[c, :, pl.ds(512 * m, 512)]) for m, src in enumerate(proj_src)
    )
    load(1, (g1_hbm, g1))
    load(2, *first_pairs)
    load(3, (wd1_hbm, wd1.at[rows_c]))
    small_pairs = (
        (gm_hbm, gm), (g2_hbm, g2), (hdl_hbm, hdl), (dib_hbm, dib), (dex_hbm, dex),
        (hng_hbm, hng), (wstr_hbm.at[:, rows_me], wstr), (wdec_hbm.at[:, rows_me], wdec),
    )
    for i, pair in enumerate(small_pairs):
        load(9 + i, pair)
    load(4, *proj_pairs)
    load(5, (state_hbm, state))
    load(6, (wo_hbm, wo.at[c]))
    load(7, *second_pairs)
    load(8, (wd2_hbm, wd2.at[rows_c]))

    loaded(0, tok)
    packed = []
    all_rows = tok[...].astype(F32).T
    for t in (0, 1):
        rows = all_rows[64 * t : 64 * t + 64]
        packed.append(jnp.concatenate([rows[:32], rows[32:]], axis=1).astype(BF16))
        s1[t] = packed[t]
    r1[me, c] = jnp.where(c == 0, packed[0], packed[1])

    pl.semaphore_wait(barrier, 31)

    for n in range(15):
        for t in (0, 1):
            remote(
                s1.at[t], r1.at[me, c], ss1, rs1.at[z], chip_to(n), t
            ).start()
    remote(s1.at[other], r1.at[me, c], sp.at[0], rp.at[0], me, other).start()

    def share(i, *pairs):
        for src, dst in pairs:
            remote(src, dst, wsend_sem.at[i], wrecv_sem.at[i], me, other).start()

    def shared(i, ref):
        remote(ref, ref, wsend_sem.at[i], wrecv_sem.at[i], me, other).wait_recv()

    def sent(ref, sem):
        remote(ref, ref, sem, rp.at[0], me, other).wait_send()

    def received(ref, sem):
        remote(ref, ref, sp.at[0], sem, me, other).wait_recv()

    share(0, *first_pairs)
    share(1, (wd1_hbm, wd1.at[rows_c]))
    share(2, *proj_pairs)

    lane = lax.broadcasted_iota(jnp.int32, (32, 128), 1)
    low = lane < 64

    def across(lhs, rhs):
        return lax.dot_general(
            lhs, rhs, (((1,), (1,)), ((), ())), preferred_element_type=F32
        )

    def swap(v):
        return pltpu.roll(v, 64, 1)

    def ffn_hidden(order, arrived, get, gain, w):
        squares = jnp.zeros((64, 128), F32)
        acc = None
        for g in order:
            arrived(g)
            parts = []
            for j in range(4 * g, 4 * g + 4):
                x = get(j)
                squares = squares + x * x
                parts.append((x * gain[j : j + 1, :]).astype(BF16))
            lhs = jnp.concatenate(parts, axis=1)
            cs = slice(512 * g, 512 * (g + 1))
            rhs = jnp.concatenate([w[k, :, cs] for k in (0, 1)], axis=0)
            d = across(lhs, rhs)
            acc = d if acc is None else acc + d
        scale = lax.rsqrt(jnp.sum(squares, axis=1, keepdims=True) * (1.0 / 2048) + EPS)
        gate = acc[:, :352] * scale
        return (jax.nn.silu(gate) * (acc[:, 352:] * scale)).astype(BF16)

    def ffn_down(hidden, w_down, emit):
        for group in SEND_GROUPS:
            cols = [pl.ds(pl.multiple_of(chip_to(n) * 128, 128), 128) for n in group]
            rhs = jnp.concatenate([w_down[:, cs] for cs in cols], axis=1)
            total = jnp.dot(hidden, rhs, preferred_element_type=F32)
            for i, n in enumerate(group):
                emit(n, total[:, 128 * i : 128 * (i + 1)])

    def from_row(g, ref, sems):
        @pl.when(z == g)
        def _():
            received(ref.at[pl.ds(0, 3)], sems.at[g])

        @pl.when(z != g)
        def _():
            received(ref.at[pl.ds(0, 4)], sems.at[g])

    def arrived1(g):
        from_row(g, r1, rs1)

    def get1(n):
        b0 = r1[n, 0].astype(F32)
        b1 = r1[n, 1].astype(F32)
        top = jnp.where(low, b0, swap(b1))
        bottom = jnp.where(low, swap(b0), b1)
        x = jnp.concatenate([top, bottom], axis=0)
        return x

    loaded(1, g1)
    loaded(2, w1.at[:, rows_c])
    shared(0, w1.at[:, rows_other])
    received(r1.at[me, other], rp.at[0])
    hidden1 = ffn_hidden((2, 3, 1, 0), arrived1, get1, g1, w1)
    own_tokens = get1(me)

    loaded(3, wd1.at[rows_c])
    shared(1, wd1.at[rows_other])
    own2 = []

    def emit2(n, block):
        if n == OWN:
            own2.append(block)
            return
        s2[n] = block.astype(BF16)
        remote(s2.at[n], r2.at[n], ss2, rs2.at[n // 8], chip_to(n), c).start()

    ffn_down(hidden1, wd1, emit2)

    share(3, (wo_hbm, wo.at[c]))

    for i, (_, dst) in enumerate(small_pairs):
        loaded(9 + i, dst)
    loaded(4, wp.at[c])
    shared(2, wp.at[other])

    total = own2[0]
    for n in range(14, -1, -1):
        if n == 14:
            received(r2.at[pl.ds(8, 7)], rs2.at[1])
        if n == 7:
            received(r2.at[pl.ds(0, 8)], rs2.at[0])
        total = total + r2[n].astype(F32)
    first = (own_tokens + 0.5 * total).astype(BF16)
    first32 = first.astype(F32)

    scaled = (first32 * gm[pl.ds(me, 1), :]).astype(BF16)
    strength = across(scaled, wstr[...])
    decay = across(scaled, wdec[...])
    sum_sq = jnp.sum(first32 * first32, axis=1, keepdims=True)
    extras = jnp.concatenate([strength, decay, sum_sq, jnp.zeros((64, 15), F32)], axis=1)
    extras_hi = extras.astype(BF16)
    extras_lo = (extras - extras_hi.astype(F32)).astype(BF16)
    extras = jnp.concatenate([extras_hi, extras_lo, jnp.zeros((64, 64), BF16)], axis=1)
    for i in range(8):
        sx[i] = extras[8 * i : 8 * i + 8]
    stays = c == my_half

    def to_owners(t, send, source_of, target, recv, own):
        for k in range(8):
            i = (me + 5 + k) % 8
            chip = 8 * c + i
            is_self = jnp.logical_and(chip == me, c == t)

            @pl.when(jnp.logical_not(is_self))
            def _():
                remote(source_of(i), target.at[me], send, recv, chip, t).start()

            @pl.when(is_self)
            def _():
                target[me] = own(i)

    def from_owners(ref, sem):
        @pl.when(stays)
        def _():
            received(ref.at[pl.ds(0, 15)], sem)

        @pl.when(jnp.logical_not(stays))
        def _():
            received(ref, sem)

    for part in (0, 1):
        for t in (0, 1):
            proj = jnp.dot(
                scaled, wp[t, :, 1024 * part : 1024 * (part + 1)], preferred_element_type=F32
            )
            for i in range(8):
                rows = slice(8 * i, 8 * i + 8)
                s3[part, t, i] = jnp.concatenate(
                    [proj[rows, :512], proj[rows, 512:]], axis=0
                ).astype(BF16)
            to_owners(
                t,
                ss3.at[part],
                lambda i: s3.at[part, t, i],
                r3.at[part],
                rs3.at[part],
                lambda i: s3[part, t, i],
            )
            if part == 0:
                to_owners(t, ssx, lambda i: sx.at[i], rx, rsx, lambda i: sx[i])

    loaded(5, state)
    for h in range(4):
        for s in range(8):
            stack[h // 2, 128 * s : 128 * (s + 1), 128 * (h % 2) : 128 * (h % 2 + 1)] = state[
                s, h
            ].astype(BF16)

    from_owners(r3.at[0], rs3.at[0])
    from_owners(rx, rsx)

    def summed_rows(ref):
        total = ref[0].astype(F32)
        for j in range(1, 16):
            total = total + ref[j].astype(F32)
        return total

    ex = summed_rows(rx)
    ex = ex + pltpu.roll(ex, 96, 1)
    factor = lax.rsqrt(ex[:, 16:17] * (1.0 / 2048) + EPS)
    ex = ex * factor
    summed = summed_rows(r3.at[0])
    core0 = c == 0
    extra_log = dex[...].T
    queries, keys, values, gates, betas, rates = [], [], [], [], [], []

    def unit(u):
        return u * lax.rsqrt(jnp.sum(u * u, axis=1, keepdims=True) + EPS)

    for h in range(4):
        lanes = slice(128 * h, 128 * (h + 1))
        queries.append(unit(jax.nn.silu(summed[:8, lanes] * factor)) * 128 ** (-0.5))
        keys.append(unit(jax.nn.silu(summed[8:, lanes] * factor)))
        betas.append(jax.nn.sigmoid(jnp.where(core0, ex[:, h : h + 1], ex[:, h + 4 : h + 5])))
        decay_in = jnp.where(core0, ex[:, h + 8 : h + 9], ex[:, h + 12 : h + 13])
        bias = jnp.where(core0, dib[:, h : h + 1], dib[:, h + 4 : h + 5])
        log_rate = jnp.where(core0, hdl[:, h : h + 1], hdl[:, h + 4 : h + 5])
        v = decay_in + bias
        softplus = jnp.maximum(v, 0.0) + jnp.log1p(jnp.exp(-jnp.abs(v)))
        rates.append(jnp.exp(extra_log[:, h : h + 1] - jnp.exp(log_rate) * softplus))
    row_seq = lax.broadcasted_iota(jnp.int32, (64, 128), 0) % 8
    recalls, reads = [], []
    for pair in (0, 1):
        rows = keys[2 * pair : 2 * pair + 2] + queries[2 * pair : 2 * pair + 2]
        rows = jnp.concatenate(rows, axis=0)
        high = rows.astype(BF16).astype(F32)
        rows = jnp.concatenate([high, rows - high], axis=0)
        lhs = jnp.concatenate(
            [jnp.where(row_seq == s, rows, 0.0) for s in range(8)], axis=1
        ).astype(BF16)
        both = jnp.dot(lhs, stack[pair], preferred_element_type=F32)
        both = both[:32] + both[32:]
        recalls += [both[:8, :128], both[8:16, 128:]]
        reads += [both[16:24, :128], both[24:, 128:]]
    from_owners(r3.at[1], rs3.at[1])
    summed = summed_rows(r3.at[1])
    for h in range(4):
        lanes = slice(128 * h, 128 * (h + 1))
        values.append(jax.nn.silu(summed[:8, lanes] * factor))
        gates.append(jax.nn.silu(summed[8:, lanes] * factor))
    heads, corrections = [], []
    for h in range(4):
        corr = betas[h] * (values[h] - rates[h] * recalls[h])
        corrections.append(corr)
        key_query = jnp.sum(keys[h] * queries[h], axis=1, keepdims=True)
        read = rates[h] * reads[h] + key_query * corr
        norm = lax.rsqrt(jnp.sum(read * read, axis=1, keepdims=True) * (1.0 / 128) + EPS)
        heads.append(read * norm * hng[...] * gates[h])
    message = jnp.concatenate(
        [jnp.concatenate(heads[:2], axis=1), jnp.concatenate(heads[2:], axis=1)], axis=0
    ).astype(BF16)
    s4[...] = message

    slot = me % 8
    for n in range(15):
        remote(s4, r4.at[c, slot], ss4, rs4.at[c], chip_to(n), my_half).start()

    @pl.when(jnp.logical_not(stays))
    def _():
        remote(s4, r4.at[c, slot], ss4, rs4.at[c], me, other).start()

    @pl.when(stays)
    def _():
        r4[c, slot] = message

    share(4, *second_pairs)
    share(5, (wd2_hbm, wd2.at[rows_c]))

    columns = jnp.concatenate(keys + [jnp.zeros((96, 128), F32)], axis=0).T
    for h in range(4):
        for s in range(8):
            m = 8 * h + s
            new_ref[s, h] = (
                state[s, h] * rates[h][s : s + 1, :]
                + columns[:, m : m + 1] * corrections[h][s : s + 1, :]
            )

    loaded(6, wo.at[c])
    shared(3, wo.at[other])

    @pl.when(stays)
    def _():
        received(r4.at[c, pl.ds(0, 7)], rs4.at[c])

    @pl.when(jnp.logical_not(stays))
    def _():
        received(r4.at[c], rs4.at[c])

    received(r4.at[other], rs4.at[other])
    mixer = jnp.zeros((64, 128), F32)
    for t in (0, 1):
        rows = []
        for i in range(8):
            part = r4[t, i].astype(F32)
            rows.append(jnp.concatenate([part[:8], part[8:]], axis=1))
        lhs = jnp.concatenate(rows, axis=0).astype(BF16)
        half = jnp.dot(lhs, wo[t], preferred_element_type=F32)
        mixer = mixer + half.astype(BF16).astype(F32)
    second = (first32 + mixer).astype(BF16)
    second32 = second.astype(F32)

    s5[...] = second
    r5[me] = second
    for n in range(15):
        remote(s5, r5.at[me], ss5, rs5.at[z], chip_to(n), c).start()

    def pack(block):
        upper, lower = block[:32], block[32:]
        return (
            jnp.where(low, upper, swap(lower)).astype(BF16),
            jnp.where(low, swap(upper), lower).astype(BF16),
        )

    p0, p1 = pack(second32)
    s7[0] = p0
    s7[1] = p1
    r7[c] = jnp.where(core0, p0, p1)
    remote(s7.at[other], r7.at[c], sp.at[1], rp.at[1], me, other).start()

    def arrived5(g):
        from_row(g, r5, rs5)

    def get5(n):
        return r5[n].astype(F32)

    loaded(7, w2.at[:, rows_c])
    shared(4, w2.at[:, rows_other])
    hidden2 = ffn_hidden((1, 2, 3, 0), arrived5, get5, g2, w2)
    loaded(8, wd2.at[rows_c])
    shared(5, wd2.at[rows_other])

    def emit6(n, block):
        packs = pack(block)
        for t in (0, 1):
            s6[n, t] = packs[t]
        if n == OWN:
            r6[OWN, c] = jnp.where(core0, packs[0], packs[1])
            remote(s6.at[OWN, other], r6.at[OWN, c], sp.at[2], rp.at[2], me, other).start()
            return
        for t in (0, 1):
            remote(s6.at[n, t], r6.at[n, c], ss6, rs6.at[n // 8], chip_to(n), t).start()

    ffn_down(hidden2, wd2, emit6)

    received(r7.at[other], rp.at[1])
    received(r6.at[OWN, other], rp.at[2])
    totals = [r6[OWN, t].astype(F32) for t in (0, 1)]
    for n in range(14, -1, -1):
        if n == 14:
            received(r6.at[pl.ds(8, 7)], rs6.at[1])
        if n == 7:
            received(r6.at[pl.ds(0, 8)], rs6.at[0])
        for t in (0, 1):
            totals[t] = totals[t] + r6[n, t].astype(F32)
    rows = []
    for t in (0, 1):
        value = r7[t].astype(F32) + 0.5 * totals[t]
        rows += [value, swap(value)]
    out_ref[...] = jnp.concatenate(rows, axis=0).T[:64].astype(BF16)
    sent(r1.at[pl.ds(0, 15)], ss1)
    sent(s1.at[0], sp.at[0])
    for i, ref in (
        (0, w1.at[:, rows_c]), (1, wd1.at[rows_c]), (2, wp.at[c]), (3, wo.at[c]),
        (4, w2.at[:, rows_c]), (5, wd2.at[rows_c]),
    ):
        sent(ref, wsend_sem.at[i])
    sent(s2, ss2)

    @pl.when(stays)
    def _():
        for part in (0, 1):
            sent(r3.at[part, pl.ds(0, 15)], ss3.at[part])
        sent(rx.at[pl.ds(0, 15)], ssx)
        sent(r6.at[pl.ds(0, 15), 0], ss4)

    @pl.when(jnp.logical_not(stays))
    def _():
        for part in (0, 1):
            sent(r3.at[part], ss3.at[part])
        sent(rx, ssx)
        sent(r4, ss4)

    sent(r5.at[pl.ds(0, 15)], ss5)
    sent(s7.at[0], sp.at[1])

    sent(r6.at[pl.ds(0, 15)], ss6)
    sent(s6.at[0, 0], sp.at[2])


def write_out(out_ref, new_ref, out_hbm, new_hbm, sem):
    copies = [pltpu.make_async_copy(out_ref, out_hbm, sem.at[8])]
    copies += [pltpu.make_async_copy(new_ref.at[s], new_hbm.at[s], sem.at[s]) for s in range(8)]
    for copy in copies:
        copy.start()
    for copy in copies:
        copy.wait()


def shards(
    tokens, first_norm_gain, first_gate_weight, first_up_weight, first_down_weight,
    mixer_norm_gain, query_weight, key_weight, value_weight, output_gate_weight,
    strength_weight, decay_weight, head_decay_log, decay_input_bias, decay_extra_log,
    head_norm_gain, state, mixer_output_weight,
    second_norm_gain, second_gate_weight, second_up_weight, second_down_weight,
):
    vm = pltpu.VMEM
    dma = pltpu.SemaphoreType.DMA
    scratch = [
        vm((64, 128), BF16), vm((16, 128), F32), vm((16, 128), F32), vm((16, 128), F32),
        vm((1, 8), F32), vm((1, 8), F32), vm((4, 8), F32), vm((1, 128), F32),
        vm((8, 128), BF16), vm((8, 128), BF16),
        vm((2, 352, 2048), BF16), vm((352, 2048), BF16),
        vm((2, 352, 2048), BF16), vm((352, 2048), BF16),
        vm((2, 128, 2048), BF16), vm((2, 512, 128), BF16), vm((8, 4, 128, 128), F32),
        vm((2, 32, 128), BF16), vm((16, 2, 32, 128), BF16),
        vm((15, 64, 128), BF16), vm((15, 64, 128), BF16),
        vm((2, 2, 8, 16, 512), BF16), vm((2, 16, 16, 512), BF16),
        vm((8, 8, 128), BF16), vm((16, 8, 128), BF16),
        vm((16, 256), BF16), vm((2, 8, 16, 256), BF16),
        vm((64, 128), BF16), vm((16, 64, 128), BF16),
        vm((16, 2, 32, 128), BF16), vm((16, 2, 32, 128), BF16),
        vm((2, 32, 128), BF16), vm((2, 32, 128), BF16),
        vm((2, 1024, 256), BF16),
        dma((17,)), dma((6,)), dma((6,)),
        dma, dma((4,)), dma, dma((2,)), dma((2,)), dma((2,)), dma, dma, dma, dma((2,)), dma, dma((4,)), dma, dma((2,)),
        dma((3,)), dma((3,)),
    ]
    out, new_state = pl.pallas_call(
        kernel,
        out_shape=(
            pltpu.VMEM((64, 128), BF16),
            pltpu.VMEM((8, 4, 128, 128), F32),
        ),
        in_specs=[pl.BlockSpec(memory_space=pltpu.HBM)] * 22,
        out_specs=[pl.BlockSpec(memory_space=pltpu.VMEM)] * 2,
        scratch_shapes=scratch,
        compiler_params=pltpu.CompilerParams(
            collective_id=0, has_side_effects=True, vmem_limit_bytes=64900000
        ),
        cost_estimate=pl.CostEstimate(
            flops=10**9, bytes_accessed=10**7, transcendentals=10**5
        ),
    )(
        tokens.T, first_norm_gain.reshape(16, 128), first_gate_weight.T, first_up_weight.T,
        first_down_weight, mixer_norm_gain.reshape(16, 128), query_weight, key_weight,
        value_weight, output_gate_weight, strength_weight.T, decay_weight.T,
        head_decay_log.reshape(1, 8), decay_input_bias.reshape(1, 8), decay_extra_log.T,
        head_norm_gain.reshape(1, 128), state, mixer_output_weight,
        second_norm_gain.reshape(16, 128), second_gate_weight.T, second_up_weight.T,
        second_down_weight,
    )
    out, new_state = pl.pallas_call(
        write_out,
        out_shape=(
            jax.ShapeDtypeStruct((64, 128), BF16),
            jax.ShapeDtypeStruct((8, 4, 128, 128), F32),
        ),
        in_specs=[pl.BlockSpec(memory_space=pltpu.VMEM)] * 2,
        out_specs=[pl.BlockSpec(memory_space=pl.ANY)] * 2,
        scratch_shapes=[dma((9,))],
        compiler_params=pltpu.CompilerParams(vmem_limit_bytes=2**22),
    )(out, new_state)
    return (out.T, new_state)


def solution(mesh):
    placed = (
        P("dp", ("kv", "tp")), P(), P(None, ("kv", "tp")), P(None, ("kv", "tp")),
        P(("kv", "tp"), None), P(), P("kv", "tp"), P("kv", "tp"), P("kv", "tp"),
        P("kv", "tp"), P(), P(), P(), P(), P(("dp", "kv"), "tp"), P(),
        P(("dp", "kv"), "tp", None, None), P("tp", "kv"), P(), P(None, ("kv", "tp")),
        P(None, ("kv", "tp")), P(("kv", "tp"), None),
    )
    return jax.shard_map(
        shards,
        mesh=mesh,
        in_specs=placed,
        out_specs=(P("dp", ("kv", "tp")), P(("dp", "kv"), "tp", None, None)),
        check_vma=False,
    )
```
